128 devices in a mesh: dp: 4 (over x), kv: 16 (over z, y), tp: 2 (over core).
Axes of the slice: x: 4, y: 4, z: 4, core: 2. Of those that a mesh axis runs over, the one named last changes fastest.
Arguments:
- tokens: bfloat16 [512, 2048], P('dp', ('kv', 'tp')), may hold values from -100 to 100
- delta_state: float32 [512, 8, 128, 128], P(('dp', 'kv'), 'tp'), may hold values from -0.6 to 0.6
- gain_in: bfloat16 [2048], P('kv'), may hold values from 0.099609375 to 1.8984375
- w_query: bfloat16 [2048, 1024], P('kv', 'tp'), may hold values from -0.125 to 0.125
- w_key: bfloat16 [2048, 1024], P('kv', 'tp'), may hold values from -0.125 to 0.125
- w_value: bfloat16 [2048, 1024], P('kv', 'tp'), may hold values from -0.125 to 0.125
- w_out_gate: bfloat16 [2048, 1024], P('kv', 'tp'), may hold values from -0.125 to 0.125
- w_beta: bfloat16 [2048, 8], P('kv'), may hold values from -0.125 to 0.125
- w_decay: bfloat16 [2048, 8], P('kv'), may hold values from -0.125 to 0.125
- decay_rate: float32 [8], P('tp'), may hold values from 0.05 to 3
- head_gain: float32 [128], replicated, may hold values from 0.1 to 1.9
- w_mix: bfloat16 [1024, 2048], P('tp', 'kv'), may hold values from -0.1875 to 0.1875
- gain_mid: bfloat16 [2048], P('kv'), may hold values from 0.099609375 to 1.8984375
- w_gate: bfloat16 [2048, 5632], P('tp', 'kv'), may hold values from -0.125 to 0.125
- w_up: bfloat16 [2048, 5632], P('tp', 'kv'), may hold values from -0.125 to 0.125
- w_down: bfloat16 [5632, 2048], P('kv', 'tp'), may hold values from -0.078125 to 0.078125
Outputs:
- layer_out: bfloat16 [512, 2048], P('dp', ('kv', 'tp'))
- next_state: float32 [512, 8, 128, 128], P(('dp', 'kv'), 'tp')
The draws below stay inside these ranges and needn't reach their ends.
All inputs are finite; a program needn't handle non-finite values.
Results may differ from the reference program's by a relative error of at most 0.0095.
Values may be sent and summed in bfloat16 or wider, within the bound.
No kernel may reach another device: no remote copies, remote signals or barrier semaphores. Data moves between devices by JAX's collectives and lax.ppermute only.
A program may use at most 64 MiB of HBM per device.

```python
import math
import jax
import jax.numpy as jnp
from jax import lax

D = 2048
HEADS = 8
HEAD_DIM = 128
FF = 5632
WIDTH = 1024
SEQS = 512
FEAT_DEV = 64
N_KV = 16
N_TP = 2


def draw_tokens(key, part):
    keys = jax.random.split(jax.random.fold_in(key, 7), 3)
    column_pos = jnp.arange(D, dtype=jnp.float32) / max(D - 1, 1)
    core_of = (jnp.arange(D) // FEAT_DEV % N_TP).astype(jnp.float32)
    rough = jax.random.uniform(keys[0], (D,), jnp.float32, 0.7, 1.4)
    column_scale = jnp.exp(jnp.log(3.0) * column_pos + jnp.log(3.0) * core_of) * rough
    row_scale = jnp.exp(jax.random.uniform(keys[1], (SEQS, 1), jnp.float32, jnp.log(0.5), jnp.log(2.0)))
    base = jnp.clip(jax.random.normal(keys[2], (SEQS, D), jnp.float32), -4.0, 4.0)
    values = jnp.clip(base * row_scale * column_scale[None, :], -96.0, 96.0)
    return values.astype(jnp.bfloat16)


def block_scale(own_key, extent, pieces, least, high):
    def one(position, blocks):
        heights = jax.random.uniform(jax.random.fold_in(jax.random.fold_in(own_key, 6), position), (blocks,), jnp.float32, least / len(pieces), high / len(pieces))
        return jnp.repeat(jnp.exp(heights), extent[position] // blocks).reshape((-1,) + (1,) * (len(extent) - position - 1))

    level = one(*pieces[0])
    for cut in pieces[1:]:
        level = level * one(*cut)
    return level


def scatter_about(stream_key, shape, spread, most, cuts=(), kind=jnp.bfloat16):
    drawn = jax.random.normal(stream_key, shape, jnp.float32) * spread
    if len(cuts) > 0:
        drawn = block_scale(stream_key, shape, cuts, -0.22, 0.18) * drawn
    return jnp.clip(drawn, min=-most, max=most).astype(kind)


def setup_inputs(seed: int = 0) -> dict:
    arg_keys = jax.random.split(jax.random.key(seed), 17)
    tokens = draw_tokens(jax.random.fold_in(arg_keys[16], 71), 0)
    delta_state = scatter_about(arg_keys[1], (SEQS, HEADS, HEAD_DIM, HEAD_DIM), 0.1, 0.6, ((0, 64), (1, 2)), jnp.float32)
    gain_in = jnp.clip(1.0 + 0.18 * jax.random.normal(arg_keys[2], (D,), jnp.float32), 0.099609375, 1.8984375).astype(jnp.bfloat16)
    w_query = scatter_about(arg_keys[3], (D, WIDTH), D ** -0.5, 0.125, ((0, 16), (1, 2)))
    w_key = scatter_about(arg_keys[4], (D, WIDTH), D ** -0.5, 0.125, ((0, 16), (1, 2)))
    w_value = scatter_about(arg_keys[5], (D, WIDTH), D ** -0.5, 0.125, ((0, 16), (1, 2)))
    w_out_gate = scatter_about(arg_keys[6], (D, WIDTH), D ** -0.5, 0.125, ((0, 16), (1, 2)))
    w_beta = scatter_about(arg_keys[7], (D, HEADS), D ** -0.5, 0.125, ((0, 16),))
    w_decay = scatter_about(arg_keys[8], (D, HEADS), D ** -0.5, 0.125, ((0, 16),))
    decay_rate = jnp.clip(jnp.exp(math.log(3.0) - 4.0943445 * jax.random.uniform(arg_keys[9], (HEADS,), jnp.float32) ** block_scale(arg_keys[9], (HEADS,), ((0, 2),), -0.2, 0.2)), 0.05, 3.0)
    head_gain = jnp.clip(1.0 + 0.18 * jax.random.normal(arg_keys[10], (HEAD_DIM,), jnp.float32), 0.1, 1.9)
    w_mix = scatter_about(arg_keys[11], (WIDTH, D), WIDTH ** -0.5, 0.1875, ((0, 2), (1, 16)))
    gain_mid = jnp.clip(1.0 + 0.18 * jax.random.normal(arg_keys[12], (D,), jnp.float32), 0.099609375, 1.8984375).astype(jnp.bfloat16)
    w_gate = scatter_about(arg_keys[13], (D, FF), D ** -0.5, 0.125, ((0, 2), (1, 16)))
    w_up = scatter_about(arg_keys[14], (D, FF), D ** -0.5, 0.125, ((0, 2), (1, 16)))
    w_down = scatter_about(arg_keys[15], (FF, D), FF ** -0.5, 0.078125, ((0, 16), (1, 2)))
    return dict(tokens=tokens, delta_state=delta_state, gain_in=gain_in, w_query=w_query, w_key=w_key, w_value=w_value, w_out_gate=w_out_gate, w_beta=w_beta, w_decay=w_decay, decay_rate=decay_rate, head_gain=head_gain, w_mix=w_mix, gain_mid=gain_mid, w_gate=w_gate, w_up=w_up, w_down=w_down)


norm_epsilon = 1e-06

def unit_rows(vector):
    return vector * lax.rsqrt(lax.optimization_barrier(jnp.sum(vector * vector, axis=-1, keepdims=True)) + norm_epsilon)

def mixer_core(query_lin, key_lin, value_lin, gate_lin, beta_lin, decay_lin, delta_state, decay_rate, head_gain):
    seq_count = query_lin.shape[0]
    head_count = beta_lin.shape[1]
    shaped = lambda matrix: matrix.reshape(seq_count, head_count, HEAD_DIM)
    query = unit_rows(jax.nn.silu(shaped(query_lin))) * HEAD_DIM ** (-0.5)
    key_vec = unit_rows(jax.nn.silu(shaped(key_lin)))
    value_vec = jax.nn.silu(shaped(value_lin))
    write_rate = jax.nn.sigmoid(beta_lin)
    keep_rate = jnp.exp(-decay_rate[None, :] * jax.nn.softplus(decay_lin))
    recalled = jnp.einsum('bhkv,bhk->bhv', delta_state, key_vec, precision=lax.Precision.HIGHEST)
    correction = write_rate[..., None] * (value_vec - keep_rate[..., None] * recalled)
    next_state = keep_rate[..., None, None] * delta_state + key_vec[..., :, None] * correction[..., None, :]
    readout = jnp.einsum('bhkv,bhk->bhv', next_state, query, precision=lax.Precision.HIGHEST)
    readout = readout * lax.rsqrt(lax.optimization_barrier(jnp.mean(readout * readout, axis=-1, keepdims=True)) + norm_epsilon)
    readout = readout * head_gain * jax.nn.silu(shaped(gate_lin))
    return (readout.reshape(seq_count, head_count * HEAD_DIM).astype(jnp.bfloat16), next_state)

def halves_product(left, right):
    span = left.shape[1] // N_TP
    total = jnp.zeros((left.shape[0], right.shape[1]), jnp.float32)
    for half_index in range(N_TP):
        partial_value = jnp.dot(left[:, half_index * span:(half_index + 1) * span], right[half_index * span:(half_index + 1) * span], preferred_element_type=jnp.float32).astype(jnp.bfloat16)
        partial_value = lax.optimization_barrier(partial_value)
        total = total + partial_value.astype(jnp.float32)
    return total

def stored_order(matrix):
    rows = matrix.shape[0]
    return jnp.transpose(matrix.reshape(rows, N_KV, N_TP, FEAT_DEV), (0, 2, 1, 3)).reshape(rows, D)

def feature_order(matrix):
    rows = matrix.shape[0]
    return jnp.transpose(matrix.reshape(rows, N_TP, N_KV, FEAT_DEV), (0, 2, 1, 3)).reshape(rows, D)

def reference(tokens, delta_state, gain_in, w_query, w_key, w_value, w_out_gate, w_beta, w_decay, decay_rate, head_gain, w_mix, gain_mid, w_gate, w_up, w_down):
    resid = tokens.astype(jnp.float32)
    row_scale = lax.rsqrt(lax.optimization_barrier(jnp.mean(resid * resid, axis=1)) + norm_epsilon)
    normed = (resid * gain_in.astype(jnp.float32)).astype(jnp.bfloat16)

    def project(weight):
        return jnp.dot(normed, weight, preferred_element_type=jnp.float32) * row_scale[:, None]
    mixed, next_state = mixer_core(project(w_query), project(w_key), project(w_value), project(w_out_gate), project(w_beta), project(w_decay), delta_state, decay_rate, head_gain)
    attn = halves_product(mixed, w_mix)
    middle = (resid + attn).astype(jnp.bfloat16)
    mid_float = middle.astype(jnp.float32)
    mid_scale = lax.rsqrt(lax.optimization_barrier(jnp.mean(mid_float * mid_float, axis=1)) + norm_epsilon)
    normed_mid = (mid_float * gain_mid.astype(jnp.float32)).astype(jnp.bfloat16)
    normed_stored = stored_order(normed_mid)
    gate_part = jnp.dot(normed_stored, w_gate, preferred_element_type=jnp.float32) * mid_scale[:, None]
    up_part = jnp.dot(normed_stored, w_up, preferred_element_type=jnp.float32) * mid_scale[:, None]
    activated = (jax.nn.silu(gate_part) * up_part).astype(jnp.bfloat16)
    down_part = feature_order(jnp.dot(activated, w_down, preferred_element_type=jnp.float32))
    layer_out = (mid_float + down_part).astype(jnp.bfloat16)
    return (layer_out, next_state)
```

```python
import jax
import jax.numpy as jnp
from jax import lax
from jax.sharding import Mesh
from jax.sharding import PartitionSpec as P

D = 2048
HEAD_DIM = 128
KV = ("kv_0", "kv_1")
KV_TP = ("kv_0", "kv_1", "tp")
DP_KV = ("dp", "kv_0", "kv_1")


norm_epsilon = 1e-06


def from_everyone(array, axis):
    copies = jnp.broadcast_to(array, (lax.axis_size(axis), *array.shape))
    return lax.all_to_all(copies, axis, split_axis=0, concat_axis=0, tiled=True)


def from_other_core(array):
    return lax.ppermute(array, "tp", [(0, 1), (1, 0)])


def two_halves(value):
    high = value.astype(jnp.bfloat16)
    low = (value - high.astype(jnp.float32)).astype(jnp.bfloat16)
    return high, low


def unit_rows(vector):
    return vector * lax.rsqrt(jnp.sum(vector * vector, axis=-1, keepdims=True) + norm_epsilon)


def mixer_core(
    query_lin, key_lin, value_lin, gate_lin, beta_lin, decay_lin, delta_state, decay_rate, head_gain
):
    seq_count = query_lin.shape[0]
    head_count = beta_lin.shape[1]
    shaped = lambda matrix: matrix.reshape(seq_count, head_count, HEAD_DIM)
    query = unit_rows(jax.nn.silu(shaped(query_lin))) * HEAD_DIM ** (-0.5)
    key_vec = unit_rows(jax.nn.silu(shaped(key_lin)))
    value_vec = jax.nn.silu(shaped(value_lin))
    write_rate = jax.nn.sigmoid(beta_lin)
    keep_rate = jnp.exp(-decay_rate[None, :] * jax.nn.softplus(decay_lin))
    recalled = jnp.einsum("bhkv,bhk->bhv", delta_state, key_vec)
    asked = jnp.einsum("bhkv,bhk->bhv", delta_state, query)
    correction = write_rate[..., None] * (value_vec - keep_rate[..., None] * recalled)
    overlap = jnp.sum(key_vec * query, axis=-1, keepdims=True)
    readout = keep_rate[..., None] * asked + overlap * correction
    readout = readout * lax.rsqrt(
        jnp.mean(readout * readout, axis=-1, keepdims=True) + norm_epsilon
    )
    readout = readout * head_gain * jax.nn.silu(shaped(gate_lin))
    next_state = (
        keep_rate[..., None, None] * delta_state + key_vec[..., :, None] * correction[..., None, :]
    )
    return (readout.reshape(seq_count, head_count * HEAD_DIM).astype(jnp.bfloat16), next_state)


def local(
    tokens,
    delta_state,
    gain_in,
    w_query,
    w_key,
    w_value,
    w_out_gate,
    w_beta,
    w_decay,
    decay_rate,
    head_gain,
    w_mix,
    gain_mid,
    w_gate,
    w_up,
    w_down,
):
    group_size = lax.axis_size(KV)
    core_pos = lax.axis_index("tp")
    on_first = core_pos == 0
    all_rows = tokens.shape[0]
    own_rows = all_rows // group_size
    feature_count = tokens.shape[1]
    head_count = w_query.shape[1] // HEAD_DIM
    width_dev = w_query.shape[1]
    token_float = tokens.astype(jnp.float32)
    other_tokens = from_other_core(tokens)
    whole_rows = jnp.concatenate(
        [
            jnp.where(on_first, tokens, other_tokens),
            jnp.where(on_first, other_tokens, tokens),
        ],
        axis=1,
    ).astype(jnp.float32)
    normed = (whole_rows * gain_in.astype(jnp.float32)).astype(jnp.bfloat16)
    squares = two_halves(jnp.sum(whole_rows * whole_rows, axis=1, keepdims=True))
    beta_cols = lax.dynamic_slice_in_dim(w_beta, core_pos * head_count, head_count, 1)
    decay_cols = lax.dynamic_slice_in_dim(w_decay, core_pos * head_count, head_count, 1)
    results = [
        jnp.dot(normed, weight, preferred_element_type=jnp.float32).astype(jnp.bfloat16)
        for weight in (w_query, w_key, w_value, w_out_gate, beta_cols, decay_cols)
    ]
    summand = jnp.concatenate([*results, *squares], axis=1)
    summand = summand.reshape(group_size, own_rows, summand.shape[1])
    pieces = lax.all_to_all(summand, KV, 0, 0, tiled=True)
    projected = jnp.sum(pieces.astype(jnp.float32), axis=0)
    gates_at = 4 * width_dev
    squares_at = gates_at + 2 * head_count
    square_total = projected[:, squares_at : squares_at + 1] + projected[:, squares_at + 1 :]
    row_scale = lax.rsqrt(square_total / D + norm_epsilon)
    projected = projected * row_scale
    mixed, next_state = mixer_core(
        projected[:, :width_dev],
        projected[:, width_dev : 2 * width_dev],
        projected[:, 2 * width_dev : 3 * width_dev],
        projected[:, 3 * width_dev : 4 * width_dev],
        projected[:, gates_at : gates_at + head_count],
        projected[:, gates_at + head_count : squares_at],
        delta_state,
        decay_rate,
        head_gain,
    )
    mixed_rows = from_everyone(mixed, KV).reshape(all_rows, width_dev)
    attn_part = jnp.dot(mixed_rows, w_mix, preferred_element_type=jnp.float32)
    own_part = lax.dynamic_slice_in_dim(attn_part, core_pos * feature_count, feature_count, 1)
    sent_part = lax.dynamic_slice_in_dim(
        attn_part, (1 - core_pos) * feature_count, feature_count, 1
    ).astype(jnp.bfloat16)
    attn = own_part + from_other_core(sent_part).astype(jnp.float32)
    middle_float = (token_float + attn).astype(jnp.bfloat16).astype(jnp.float32)
    mid_squares = two_halves(jnp.sum(middle_float * middle_float, axis=1, keepdims=True))
    gain_own = lax.dynamic_slice_in_dim(gain_mid, core_pos * feature_count, feature_count, 0)
    normed_own = (middle_float * gain_own.astype(jnp.float32)).astype(jnp.bfloat16)
    sent = jnp.concatenate([normed_own, *mid_squares], axis=1)
    received = from_everyone(sent, KV)
    normed_half = jnp.moveaxis(received[:, :, :feature_count], 0, 1).reshape(
        all_rows, group_size * feature_count
    )
    half_total = jnp.sum(received[:, :, feature_count:].astype(jnp.float32), axis=(0, 2))
    hidden_dev = w_gate.shape[1]
    summand = jnp.concatenate(
        [
            jnp.dot(normed_half, w_gate, preferred_element_type=jnp.float32),
            jnp.dot(normed_half, w_up, preferred_element_type=jnp.float32),
        ],
        axis=1,
    )
    gate_up = summand + from_other_core(summand.astype(jnp.bfloat16)).astype(jnp.float32)
    mid_total = half_total + from_other_core(half_total)
    mid_scale = lax.rsqrt(mid_total / D + norm_epsilon)
    gate_up = gate_up * mid_scale[:, None]
    activated = (jax.nn.silu(gate_up[:, :hidden_dev]) * gate_up[:, hidden_dev:]).astype(
        jnp.bfloat16
    )
    down_local = jnp.dot(activated, w_down, preferred_element_type=jnp.float32)
    tiles = down_local.astype(jnp.bfloat16).reshape(all_rows, group_size, feature_count)
    pieces = lax.all_to_all(jnp.moveaxis(tiles, 1, 0), KV, 0, 0, tiled=True)
    down_part = jnp.sum(pieces.astype(jnp.float32), axis=0)
    layer_out = (middle_float + down_part).astype(jnp.bfloat16)
    return (layer_out, next_state)


def solution(mesh):
    split = Mesh(
        mesh.devices.reshape(mesh.shape["dp"], 4, 4, mesh.shape["tp"]), ("dp", "kv_0", "kv_1", "tp")
    )
    in_specs = (
        P("dp", KV_TP),
        P(DP_KV, "tp", None, None),
        P(KV),
        P(KV, "tp"),
        P(KV, "tp"),
        P(KV, "tp"),
        P(KV, "tp"),
        P(KV, None),
        P(KV, None),
        P("tp"),
        P(),
        P("tp", KV),
        P(KV),
        P("tp", KV),
        P("tp", KV),
        P(KV, "tp"),
    )
    out_specs = (P("dp", KV_TP), P(DP_KV, "tp", None, None))
    return jax.shard_map(local, mesh=split, in_specs=in_specs, out_specs=out_specs, check_vma=False)
```

```python
import jax
import jax.numpy as jnp
from jax import lax
from jax.experimental import pallas as pl
from jax.experimental.pallas import tpu as pltpu
from jax.sharding import Mesh
from jax.sharding import PartitionSpec as P

D = 2048
HEAD_DIM = 128
KV = ("kv_0", "kv_1")
KV_TP = ("kv_0", "kv_1", "tp")
DP_KV = ("dp", "kv_0", "kv_1")

norm_epsilon = 1e-06
bf16 = jnp.bfloat16
f32 = jnp.float32

GROUP = 16
ROWS = 128
OWN = ROWS // GROUP
FEAT = 64
HEADS_DEV = 4
WIDTH_DEV = HEADS_DEV * HEAD_DIM
PIECE = 4 * WIDTH_DEV + 128
SQUARE_AT = 4 * WIDTH_DEV + 2 * HEADS_DEV
TALL = FEAT + 8
HIDDEN = 352
BOTH = 2 * HIDDEN

TN = (((0,), (0,)), ((), ()))
NT = (((1,), (1,)), ((), ()))


def in_vmem():
    return pl.BlockSpec(memory_space=pltpu.VMEM)


def anywhere():
    return pl.BlockSpec(memory_space=pl.ANY)


def shape(lengths, dtype):
    return jax.ShapeDtypeStruct(lengths, dtype)


def kernel(body, name, outs, in_specs, limit=12):
    single = not isinstance(outs, (list, tuple))
    return pl.pallas_call(
        body,
        out_shape=outs,
        in_specs=in_specs,
        out_specs=in_vmem() if single else [in_vmem() for _ in outs],
        name=name,
        compiler_params=pltpu.CompilerParams(vmem_limit_bytes=limit * 1024 * 1024),
    )


def silu(value):
    return value / (1.0 + jnp.exp(-value))


def high_low(value):
    high = value.astype(bf16).astype(f32)
    return high, value - high


def dot(left, right, dims=(((1,), (0,)), ((), ()))):
    return lax.dot_general(left, right, dims, preferred_element_type=f32)


def project(own_ref, other_ref, gain_ref, wq_ref, wk_ref, wv_ref, wg_ref, wb_ref, wd_ref, out_ref):
    on_first = lax.axis_index("tp") == 0
    own = own_ref[...].astype(f32)
    other = other_ref[...].astype(f32)
    rows = jnp.concatenate(
        [jnp.where(on_first, own, other), jnp.where(on_first, other, own)], axis=0
    ).T
    high, low = high_low(jnp.sum(rows * rows, axis=1, keepdims=True))
    normed = (rows * gain_ref[...].astype(f32)).astype(bf16)
    for at, ref in enumerate((wq_ref, wk_ref, wv_ref, wg_ref)):
        out_ref[:, at * WIDTH_DEV : (at + 1) * WIDTH_DEV] = dot(normed, ref[...]).astype(bf16)
    beta = wb_ref[...].astype(f32)
    decay = wd_ref[...].astype(f32)
    small = jnp.concatenate(
        [
            jnp.where(on_first, beta[:HEADS_DEV], beta[HEADS_DEV:]),
            jnp.where(on_first, decay[:HEADS_DEV], decay[HEADS_DEV:]),
            jnp.zeros((128 - 2 * HEADS_DEV, 128), f32),
        ],
        axis=0,
    ).astype(bf16)
    extra = dot(normed, small, NT)
    lane = lax.broadcasted_iota(jnp.int32, extra.shape, 1)
    extra = jnp.where(lane == 2 * HEADS_DEV, high, extra)
    extra = jnp.where(lane == 2 * HEADS_DEV + 1, low, extra)
    out_ref[:, 4 * WIDTH_DEV :] = extra.astype(bf16)


def mixer(pieces_ref, state_ref, rate_ref, head_gain_ref, mixed_ref, key_ref, correct_ref, keep_ref):
    def total(first, last):
        parts = [pieces_ref[OWN * s : OWN * (s + 1), first:last].astype(f32) for s in range(GROUP)]
        while len(parts) > 1:
            parts = [a + b for a, b in zip(parts[::2], parts[1::2])]
        return parts[0]

    small = total(4 * WIDTH_DEV, PIECE)
    square = 2 * HEADS_DEV
    row_scale = lax.rsqrt(
        (small[:, square : square + 1] + small[:, square + 1 : square + 2]) / D + norm_epsilon
    )
    small = small * row_scale
    row = lax.broadcasted_iota(jnp.int32, (OWN, HEAD_DIM), 0)
    lane = lax.broadcasted_iota(jnp.int32, (OWN, HEAD_DIM), 1)
    keeps = jnp.zeros((OWN, HEAD_DIM), f32)

    def unit(vector):
        return vector * lax.rsqrt(jnp.sum(vector * vector, axis=1, keepdims=True) + norm_epsilon)

    for h in range(HEADS_DEV):
        at = h * HEAD_DIM
        query_lin, key_lin, value_lin, gate_lin = (
            total(part * WIDTH_DEV + at, part * WIDTH_DEV + at + HEAD_DIM) * row_scale
            for part in range(4)
        )
        query = unit(silu(query_lin)) * HEAD_DIM ** (-0.5)
        key = unit(silu(key_lin))
        write_rate = 1.0 / (1.0 + jnp.exp(-small[:, h : h + 1]))
        decay = small[:, HEADS_DEV + h : HEADS_DEV + h + 1]
        softplus = jnp.maximum(decay, 0.0) + jnp.log1p(jnp.exp(-jnp.abs(decay)))
        keep = jnp.exp(-rate_ref[:, h : h + 1] * softplus)
        pair = jnp.concatenate([key, query], axis=0).astype(bf16)
        recalled = jnp.zeros((OWN, HEAD_DIM), f32)
        asked = jnp.zeros((OWN, HEAD_DIM), f32)
        for b in range(OWN):
            both = dot(pair, state_ref[b, h].astype(bf16))
            recalled = jnp.where(row == b, both[:OWN], recalled)
            asked = jnp.where(row == b, both[OWN:], asked)
        correction = write_rate * (silu(value_lin) - keep * recalled)
        readout = keep * asked + jnp.sum(key * query, axis=1, keepdims=True) * correction
        readout = readout * lax.rsqrt(
            jnp.mean(readout * readout, axis=1, keepdims=True) + norm_epsilon
        )
        mixed = (readout * head_gain_ref[...] * silu(gate_lin)).astype(bf16)
        for s in range(GROUP):
            mixed_ref[OWN * s : OWN * (s + 1), at : at + HEAD_DIM] = mixed
        key_ref[:, at : at + HEAD_DIM] = key
        correct_ref[:, at : at + HEAD_DIM] = correction
        keeps = jnp.where(lane == h, keep, keeps)
    keep_ref[...] = keeps


def update(state_ref, key_ref, correct_ref, keep_ref, after_ref, next_ref):
    del after_ref
    b = pl.program_id(0)
    pick = lax.broadcasted_iota(jnp.int32, (OWN, WIDTH_DEV), 0) == b
    key = jnp.sum(jnp.where(pick, key_ref[...], 0.0), axis=0, keepdims=True)
    correction = jnp.sum(jnp.where(pick, correct_ref[...], 0.0), axis=0, keepdims=True)
    keep = jnp.sum(jnp.where(pick[:, :HEAD_DIM], keep_ref[...], 0.0), axis=0, keepdims=True)
    for h in range(HEADS_DEV):
        at = h * HEAD_DIM
        key_column = jnp.broadcast_to(key[:, at : at + HEAD_DIM], (HEAD_DIM, HEAD_DIM)).T
        next_ref[0, h] = (
            keep[:, h : h + 1] * state_ref[0, h] + key_column * correction[:, at : at + HEAD_DIM]
        )


def mix(mixed_ref, w_ref, own_ref, sent_ref):
    on_first = lax.axis_index("tp") == 0
    part = dot(mixed_ref[...], w_ref[...]).T
    own_ref[...] = jnp.where(on_first, part[:FEAT], part[FEAT:])
    sent_ref[...] = jnp.where(on_first, part[FEAT:], part[:FEAT]).astype(bf16)


def middle_rows(tokens_ref, own_ref, other_ref, gain_ref, middle_ref, sent_ref):
    on_first = lax.axis_index("tp") == 0
    gains = jnp.broadcast_to(gain_ref[...].astype(f32), (128, 128)).T
    gain = jnp.where(on_first, gains[:FEAT], gains[FEAT:])
    middle = tokens_ref[...].astype(f32) + (own_ref[...] + other_ref[...].astype(f32))
    middle_ref[...] = middle.astype(bf16)
    middle = middle.astype(bf16).astype(f32)
    normed = (middle * gain).astype(bf16)
    high, low = high_low(jnp.sum(middle * middle, axis=0, keepdims=True))
    squares = jnp.concatenate([high, low, jnp.zeros((6, ROWS), f32)], axis=0).astype(bf16)
    for s in range(GROUP):
        sent_ref[TALL * s : TALL * s + FEAT] = normed
        sent_ref[TALL * s + FEAT : TALL * (s + 1)] = squares


def gate_up(received_ref, wg_ref, wu_ref, own_ref, sent_ref):
    rows = jnp.concatenate(
        [received_ref[TALL * s : TALL * s + FEAT] for s in range(GROUP)], axis=0
    )
    squares = sum(
        received_ref[TALL * s + FEAT : TALL * (s + 1)].astype(f32) for s in range(GROUP)
    )
    total = squares[0:1] + squares[1:2]
    high, low = high_low(total)
    for at, ref in ((0, wg_ref), (HIDDEN, wu_ref)):
        part = dot(ref[...], rows)
        own_ref[at : at + HIDDEN] = part
        sent_ref[at : at + HIDDEN] = part.astype(bf16)
    own_ref[BOTH:] = jnp.broadcast_to(total, (8, ROWS))
    sent_ref[BOTH:] = jnp.concatenate([high, low, jnp.zeros((6, ROWS), f32)], axis=0).astype(bf16)


def down(own_ref, other_ref, w_ref, after_ref, out_ref):
    del after_ref
    squares = other_ref[BOTH:].astype(f32)
    total = own_ref[BOTH : BOTH + 1] + squares[0:1] + squares[1:2]
    scale = lax.rsqrt(total / D + norm_epsilon)
    gate = (own_ref[:HIDDEN] + other_ref[:HIDDEN].astype(f32)) * scale
    up = (own_ref[HIDDEN:BOTH] + other_ref[HIDDEN:BOTH].astype(f32)) * scale
    active = (silu(gate) * up).astype(bf16)
    out_ref[...] = dot(w_ref[...], active, TN).astype(bf16)


def finish(received_ref, middle_ref, out_ref):
    parts = [received_ref[FEAT * s : FEAT * (s + 1)].astype(f32) for s in range(GROUP)]
    while len(parts) > 1:
        parts = [a + b for a, b in zip(parts[::2], parts[1::2])]
    out_ref[...] = (middle_ref[...].astype(f32) + parts[0]).astype(bf16)


def from_other_core(array):
    return lax.ppermute(array, "tp", [(0, 1), (1, 0)])


def over_group(array):
    tiles = array.reshape(GROUP, array.shape[0] // GROUP, array.shape[1])
    return lax.all_to_all(tiles, KV, 0, 0, tiled=True).reshape(array.shape)


def local(
    tokens,
    delta_state,
    gain_in,
    w_query,
    w_key,
    w_value,
    w_out_gate,
    w_beta,
    w_decay,
    decay_rate,
    head_gain,
    w_mix,
    gain_mid,
    w_gate,
    w_up,
    w_down,
):
    v, a = in_vmem(), anywhere()
    own_tokens = tokens.T
    other_tokens = from_other_core(own_tokens)
    summand = kernel(project, "project", shape((ROWS, PIECE), bf16), [v] * 9)(
        own_tokens,
        other_tokens,
        gain_in.reshape(1, 128),
        w_query,
        w_key,
        w_value,
        w_out_gate,
        w_beta.T,
        w_decay.T,
    )
    pieces = over_group(summand)
    mixed, key, correction, keep = kernel(
        mixer,
        "mixer",
        [
            shape((ROWS, WIDTH_DEV), bf16),
            shape((OWN, WIDTH_DEV), f32),
            shape((OWN, WIDTH_DEV), f32),
            shape((OWN, HEAD_DIM), f32),
        ],
        [v] * 4,
    )(pieces, delta_state, decay_rate.reshape(1, HEADS_DEV), head_gain.reshape(1, HEAD_DIM))
    mixed_rows = over_group(mixed)
    own_part, sent_part = kernel(
        mix, "mix", [shape((FEAT, ROWS), f32), shape((FEAT, ROWS), bf16)], [v] * 2
    )(mixed_rows, w_mix)
    middle, sent = kernel(
        middle_rows,
        "middle_rows",
        [shape((FEAT, ROWS), bf16), shape((GROUP * TALL, ROWS), bf16)],
        [v] * 4,
    )(own_tokens, own_part, from_other_core(sent_part), gain_mid.reshape(1, 128))
    received = over_group(sent)
    own_sum, sent_sum = kernel(
        gate_up,
        "gate_up",
        [shape((BOTH + 8, ROWS), f32), shape((BOTH + 8, ROWS), bf16)],
        [v] * 3,
    )(received, w_gate.T, w_up.T)
    block = pl.BlockSpec((1, HEADS_DEV, HEAD_DIM, HEAD_DIM), lambda b: (b, 0, 0, 0))
    next_state = pl.pallas_call(
        update,
        grid=(OWN,),
        out_shape=shape(delta_state.shape, f32),
        in_specs=[block, v, v, v, a],
        out_specs=block,
        name="update",
        compiler_params=pltpu.CompilerParams(vmem_limit_bytes=8 * 1024 * 1024),
    )(delta_state, key, correction, keep, received)
    down_local = kernel(down, "down", shape((GROUP * FEAT, ROWS), bf16), [v, v, v, a])(
        own_sum, from_other_core(sent_sum), w_down, next_state
    )
    layer_out = kernel(finish, "finish", shape((FEAT, ROWS), bf16), [v] * 2)(
        over_group(down_local), middle
    )
    return (layer_out.T, next_state)


def solution(mesh):
    split = Mesh(
        mesh.devices.reshape(mesh.shape["dp"], 4, 4, mesh.shape["tp"]), ("dp", "kv_0", "kv_1", "tp")
    )
    in_specs = (
        P("dp", KV_TP),
        P(DP_KV, "tp", None, None),
        P(KV),
        P(KV, "tp"),
        P(KV, "tp"),
        P(KV, "tp"),
        P(KV, "tp"),
        P(KV, None),
        P(KV, None),
        P("tp"),
        P(),
        P("tp", KV),
        P(KV),
        P("tp", KV),
        P("tp", KV),
        P(KV, "tp"),
    )
    out_specs = (P("dp", KV_TP), P(DP_KV, "tp", None, None))
    return jax.shard_map(local, mesh=split, in_specs=in_specs, out_specs=out_specs, check_vma=False)
```

```python
import functools

import jax
import jax.numpy as jnp
from jax import lax
from jax.experimental import pallas as pl
from jax.experimental.pallas import tpu as pltpu
from jax.sharding import Mesh
from jax.sharding import PartitionSpec as P

D = 2048
HEAD_DIM = 128
KV = ("kv_0", "kv_1")
KV_TP = ("kv_0", "kv_1", "tp")
DP_KV = ("dp", "kv_0", "kv_1")

norm_epsilon = 1e-06
bf16 = jnp.bfloat16
f32 = jnp.float32

GROUP = 16
ROWS = 128
OWN = ROWS // GROUP
FEAT = 64
HEADS_DEV = 4
WIDTH_DEV = HEADS_DEV * HEAD_DIM
PIECE = 4 * WIDTH_DEV + 128
SQUARE_AT = 4 * WIDTH_DEV + 2 * HEADS_DEV
TALL = FEAT + 8
HIDDEN = 352
BOTH = 2 * HIDDEN

TN = (((0,), (0,)), ((), ()))
NT = (((1,), (1,)), ((), ()))


def in_vmem():
    return pl.BlockSpec(memory_space=pltpu.VMEM)


def anywhere():
    return pl.BlockSpec(memory_space=pl.ANY)


def shape(lengths, dtype):
    return jax.ShapeDtypeStruct(lengths, dtype)


def kernel(body, name, outs, in_specs, limit=12):
    single = not isinstance(outs, (list, tuple))
    return pl.pallas_call(
        body,
        out_shape=outs,
        in_specs=in_specs,
        out_specs=in_vmem() if single else [in_vmem() for _ in outs],
        name=name,
        compiler_params=pltpu.CompilerParams(vmem_limit_bytes=limit * 1024 * 1024),
    )


def silu(value):
    return value / (1.0 + jnp.exp(-value))


def high_low(value):
    high = value.astype(bf16).astype(f32)
    return high, value - high


def dot(left, right, dims=(((1,), (0,)), ((), ()))):
    return lax.dot_general(left, right, dims, preferred_element_type=f32)


def project(own_ref, other_ref, gain_ref, wq_ref, wk_ref, wv_ref, wg_ref, wb_ref, wd_ref, out_ref):
    on_first = lax.axis_index("tp") == 0
    own = own_ref[...].astype(f32)
    other = other_ref[...].astype(f32)
    rows = jnp.concatenate(
        [jnp.where(on_first, own, other), jnp.where(on_first, other, own)], axis=0
    ).T
    high, low = high_low(jnp.sum(rows * rows, axis=1, keepdims=True))
    normed = (rows * gain_ref[...].astype(f32)).astype(bf16)
    for at, ref in enumerate((wq_ref, wk_ref, wv_ref, wg_ref)):
        out_ref[:, at * WIDTH_DEV : (at + 1) * WIDTH_DEV] = dot(normed, ref[...]).astype(bf16)
    beta = wb_ref[...].astype(f32)
    decay = wd_ref[...].astype(f32)
    small = jnp.concatenate(
        [
            jnp.where(on_first, beta[:HEADS_DEV], beta[HEADS_DEV:]),
            jnp.where(on_first, decay[:HEADS_DEV], decay[HEADS_DEV:]),
            jnp.zeros((128 - 2 * HEADS_DEV, 128), f32),
        ],
        axis=0,
    ).astype(bf16)
    extra = dot(normed, small, NT)
    lane = lax.broadcasted_iota(jnp.int32, extra.shape, 1)
    extra = jnp.where(lane == 2 * HEADS_DEV, high, extra)
    extra = jnp.where(lane == 2 * HEADS_DEV + 1, low, extra)
    out_ref[:, 4 * WIDTH_DEV :] = extra.astype(bf16)


def mixer(pieces_ref, state_ref, rate_ref, head_gain_ref, mixed_ref, key_ref, correct_ref, keep_ref):
    def total(first, last):
        parts = [pieces_ref[OWN * s : OWN * (s + 1), first:last].astype(f32) for s in range(GROUP)]
        while len(parts) > 1:
            parts = [a + b for a, b in zip(parts[::2], parts[1::2])]
        return parts[0]

    small = total(4 * WIDTH_DEV, PIECE)
    square = 2 * HEADS_DEV
    row_scale = lax.rsqrt(
        (small[:, square : square + 1] + small[:, square + 1 : square + 2]) / D + norm_epsilon
    )
    small = small * row_scale
    row = lax.broadcasted_iota(jnp.int32, (OWN, HEAD_DIM), 0)
    lane = lax.broadcasted_iota(jnp.int32, (OWN, HEAD_DIM), 1)
    keeps = jnp.zeros((OWN, HEAD_DIM), f32)

    def unit(vector):
        return vector * lax.rsqrt(jnp.sum(vector * vector, axis=1, keepdims=True) + norm_epsilon)

    for h in range(HEADS_DEV):
        at = h * HEAD_DIM
        query_lin, key_lin, value_lin, gate_lin = (
            total(part * WIDTH_DEV + at, part * WIDTH_DEV + at + HEAD_DIM) * row_scale
            for part in range(4)
        )
        query = unit(silu(query_lin)) * HEAD_DIM ** (-0.5)
        key = unit(silu(key_lin))
        write_rate = 1.0 / (1.0 + jnp.exp(-small[:, h : h + 1]))
        decay = small[:, HEADS_DEV + h : HEADS_DEV + h + 1]
        softplus = jnp.maximum(decay, 0.0) + jnp.log1p(jnp.exp(-jnp.abs(decay)))
        keep = jnp.exp(-rate_ref[:, h : h + 1] * softplus)
        pair = jnp.concatenate([key, query], axis=0).astype(bf16)
        recalled = jnp.zeros((OWN, HEAD_DIM), f32)
        asked = jnp.zeros((OWN, HEAD_DIM), f32)
        for b in range(OWN):
            both = dot(pair, state_ref[b, h].astype(bf16))
            recalled = jnp.where(row == b, both[:OWN], recalled)
            asked = jnp.where(row == b, both[OWN:], asked)
        correction = write_rate * (silu(value_lin) - keep * recalled)
        readout = keep * asked + jnp.sum(key * query, axis=1, keepdims=True) * correction
        readout = readout * lax.rsqrt(
            jnp.mean(readout * readout, axis=1, keepdims=True) + norm_epsilon
        )
        mixed = (readout * head_gain_ref[...] * silu(gate_lin)).astype(bf16)
        for s in range(GROUP):
            mixed_ref[OWN * s : OWN * (s + 1), at : at + HEAD_DIM] = mixed
        key_ref[:, at : at + HEAD_DIM] = key
        correct_ref[:, at : at + HEAD_DIM] = correction
        keeps = jnp.where(lane == h, keep, keeps)
    keep_ref[...] = keeps


HALF = OWN // 2


def update(first, state_ref, key_ref, correct_ref, keep_ref, after_ref, *rest):
    del after_ref
    next_ref, token_ref, made_ref, sems = rest[-4:]
    copies = []
    for b in range(HALF):
        row = first + b
        for h in range(HEADS_DEV):
            at = h * HEAD_DIM
            key = key_ref[row : row + 1, at : at + HEAD_DIM]
            key_column = jnp.broadcast_to(key, (HEAD_DIM, HEAD_DIM)).T
            made_ref[b, h] = (
                keep_ref[row : row + 1, h : h + 1] * state_ref[row, h]
                + key_column * correct_ref[row : row + 1, at : at + HEAD_DIM]
            )
        copies.append(pltpu.make_async_copy(made_ref.at[b], next_ref.at[row], sems.at[b]))
        copies[-1].start()
    token_ref[...] = jnp.zeros(token_ref.shape, f32)
    for copy in copies:
        copy.wait()


def updated(first, state, key, correction, keep, after, base=None):
    operands = [state, key, correction, keep, after] + ([] if base is None else [base])
    hbm = pl.BlockSpec(memory_space=pltpu.HBM)
    return pl.pallas_call(
        functools.partial(update, first),
        out_shape=[shape(state.shape, f32), shape((8, 128), f32)],
        in_specs=[in_vmem()] * 4 + [anywhere()] + ([] if base is None else [hbm]),
        out_specs=[hbm, in_vmem()],
        scratch_shapes=[
            pltpu.VMEM((HALF, HEADS_DEV, HEAD_DIM, HEAD_DIM), f32),
            pltpu.SemaphoreType.DMA((HALF,)),
        ],
        input_output_aliases={} if base is None else {5: 0},
        name="update",
        compiler_params=pltpu.CompilerParams(vmem_limit_bytes=12 * 1024 * 1024),
    )(*operands)


def preload(*refs):
    count = (len(refs) - 1) // 2
    sems = refs[-1]
    copies = [
        pltpu.make_async_copy(refs[i], refs[count + i], sems.at[i]) for i in range(count)
    ]
    for copy in copies:
        copy.start()
    for copy in copies:
        copy.wait()


def preloaded(*arrays):
    return pl.pallas_call(
        preload,
        out_shape=[shape(x.shape, x.dtype) for x in arrays],
        in_specs=[pl.BlockSpec(memory_space=pltpu.HBM)] * len(arrays),
        out_specs=[in_vmem() for _ in arrays],
        scratch_shapes=[pltpu.SemaphoreType.DMA((len(arrays),))],
        name="preload",
        compiler_params=pltpu.CompilerParams(vmem_limit_bytes=4 * 1024 * 1024),
    )(*(pltpu.with_memory_space_constraint(x, pltpu.HBM) for x in arrays))


def mix(mixed_ref, w_ref, own_ref, sent_ref):
    on_first = lax.axis_index("tp") == 0
    part = dot(mixed_ref[...], w_ref[...]).T
    own_ref[...] = jnp.where(on_first, part[:FEAT], part[FEAT:])
    sent_ref[...] = jnp.where(on_first, part[FEAT:], part[:FEAT]).astype(bf16)


def middle_rows(tokens_ref, own_ref, other_ref, gain_ref, after_ref, middle_ref, sent_ref):
    del after_ref
    on_first = lax.axis_index("tp") == 0
    gains = jnp.broadcast_to(gain_ref[...].astype(f32), (128, 128)).T
    gain = jnp.where(on_first, gains[:FEAT], gains[FEAT:])
    middle = tokens_ref[...].astype(f32) + (own_ref[...] + other_ref[...].astype(f32))
    middle_ref[...] = middle.astype(bf16)
    middle = middle.astype(bf16).astype(f32)
    normed = (middle * gain).astype(bf16)
    high, low = high_low(jnp.sum(middle * middle, axis=0, keepdims=True))
    squares = jnp.concatenate([high, low, jnp.zeros((6, ROWS), f32)], axis=0).astype(bf16)
    for s in range(GROUP):
        sent_ref[TALL * s : TALL * s + FEAT] = normed
        sent_ref[TALL * s + FEAT : TALL * (s + 1)] = squares


def gate_up(received_ref, wg_ref, wu_ref, own_ref, sent_ref):
    rows = jnp.concatenate(
        [received_ref[TALL * s : TALL * s + FEAT] for s in range(GROUP)], axis=0
    )
    squares = sum(
        received_ref[TALL * s + FEAT : TALL * (s + 1)].astype(f32) for s in range(GROUP)
    )
    total = squares[0:1] + squares[1:2]
    high, low = high_low(total)
    for at, ref in ((0, wg_ref), (HIDDEN, wu_ref)):
        part = dot(ref[...], rows)
        own_ref[at : at + HIDDEN] = part
        sent_ref[at : at + HIDDEN] = part.astype(bf16)
    own_ref[BOTH:] = jnp.broadcast_to(total, (8, ROWS))
    sent_ref[BOTH:] = jnp.concatenate([high, low, jnp.zeros((6, ROWS), f32)], axis=0).astype(bf16)


def down(own_ref, other_ref, w_ref, after_ref, out_ref):
    del after_ref
    squares = other_ref[BOTH:].astype(f32)
    total = own_ref[BOTH : BOTH + 1] + squares[0:1] + squares[1:2]
    scale = lax.rsqrt(total / D + norm_epsilon)
    gate = (own_ref[:HIDDEN] + other_ref[:HIDDEN].astype(f32)) * scale
    up = (own_ref[HIDDEN:BOTH] + other_ref[HIDDEN:BOTH].astype(f32)) * scale
    active = (silu(gate) * up).astype(bf16)
    out_ref[...] = dot(w_ref[...], active, TN).astype(bf16)


def finish(received_ref, middle_ref, out_ref):
    parts = [received_ref[FEAT * s : FEAT * (s + 1)].astype(f32) for s in range(GROUP)]
    while len(parts) > 1:
        parts = [a + b for a, b in zip(parts[::2], parts[1::2])]
    out_ref[...] = (middle_ref[...].astype(f32) + parts[0]).astype(bf16)


def from_other_core(array):
    return lax.ppermute(array, "tp", [(0, 1), (1, 0)])


def over_group(array):
    tiles = array.reshape(GROUP, array.shape[0] // GROUP, array.shape[1])
    return lax.all_to_all(tiles, KV, 0, 0, tiled=True).reshape(array.shape)


def local(
    tokens,
    delta_state,
    gain_in,
    w_query,
    w_key,
    w_value,
    w_out_gate,
    w_beta,
    w_decay,
    decay_rate,
    head_gain,
    w_mix,
    gain_mid,
    w_gate,
    w_up,
    w_down,
):
    v, a = in_vmem(), anywhere()
    own_tokens = tokens.T
    other_tokens = from_other_core(own_tokens)
    loaded = preloaded(
        own_tokens,
        gain_in.reshape(1, 128),
        w_query,
        w_key,
        w_value,
        w_out_gate,
        w_beta.T,
        w_decay.T,
    )
    summand = kernel(project, "project", shape((ROWS, PIECE), bf16), [v] * 9)(
        loaded[0], other_tokens, *loaded[1:]
    )
    pieces = over_group(summand)
    mixed, key, correction, keep = kernel(
        mixer,
        "mixer",
        [
            shape((ROWS, WIDTH_DEV), bf16),
            shape((OWN, WIDTH_DEV), f32),
            shape((OWN, WIDTH_DEV), f32),
            shape((OWN, HEAD_DIM), f32),
        ],
        [v] * 4,
    )(pieces, delta_state, decay_rate.reshape(1, HEADS_DEV), head_gain.reshape(1, HEAD_DIM))
    mixed_rows = over_group(mixed)
    own_part, sent_part = kernel(
        mix, "mix", [shape((FEAT, ROWS), f32), shape((FEAT, ROWS), bf16)], [v] * 2
    )(mixed_rows, w_mix)
    half_state, half_token = updated(0, delta_state, key, correction, keep, mixed_rows)
    middle, sent = kernel(
        middle_rows,
        "middle_rows",
        [shape((FEAT, ROWS), bf16), shape((GROUP * TALL, ROWS), bf16)],
        [v] * 4 + [a],
    )(loaded[0], own_part, from_other_core(sent_part), gain_mid.reshape(1, 128), half_token)
    received = over_group(sent)
    own_sum, sent_sum = kernel(
        gate_up,
        "gate_up",
        [shape((BOTH + 8, ROWS), f32), shape((BOTH + 8, ROWS), bf16)],
        [v] * 3,
    )(received, w_gate.T, w_up.T)
    next_state, token = updated(HALF, delta_state, key, correction, keep, received, half_state)
    down_local = kernel(down, "down", shape((GROUP * FEAT, ROWS), bf16), [v, v, v, a])(
        own_sum, from_other_core(sent_sum), w_down, token
    )
    layer_out = kernel(finish, "finish", shape((FEAT, ROWS), bf16), [v] * 2)(
        over_group(down_local), middle
    )
    return (layer_out.T, next_state)


def solution(mesh):
    split = Mesh(
        mesh.devices.reshape(mesh.shape["dp"], 4, 4, mesh.shape["tp"]), ("dp", "kv_0", "kv_1", "tp")
    )
    in_specs = (
        P("dp", KV_TP),
        P(DP_KV, "tp", None, None),
        P(KV),
        P(KV, "tp"),
        P(KV, "tp"),
        P(KV, "tp"),
        P(KV, "tp"),
        P(KV, None),
        P(KV, None),
        P("tp"),
        P(),
        P("tp", KV),
        P(KV),
        P("tp", KV),
        P("tp", KV),
        P(KV, "tp"),
    )
    out_specs = (P("dp", KV_TP), P(DP_KV, "tp", None, None))
    return jax.shard_map(local, mesh=split, in_specs=in_specs, out_specs=out_specs, check_vma=False)
```

```python
import jax
import jax.numpy as jnp
from jax import lax
from jax.experimental import pallas as pl
from jax.experimental.pallas import tpu as pltpu
from jax.sharding import Mesh
from jax.sharding import PartitionSpec as P


D = 2048
HEAD_DIM = 128
KV = ("kv_0", "kv_1")
KV_TP = ("kv_0", "kv_1", "tp")
DP_KV = ("dp", "kv_0", "kv_1")

norm_epsilon = 1e-06
bf16 = jnp.bfloat16
f32 = jnp.float32

GROUP = 16
ROWS = 128
OWN = ROWS // GROUP
FEAT = 64
HEADS_DEV = 4
WIDTH_DEV = HEADS_DEV * HEAD_DIM
SMALL_AT = 4 * WIDTH_DEV
TOKENS_AT = SMALL_AT + 128
PIECE = TOKENS_AT + 128
RING = 4
FEAT_RING = RING * FEAT
SEQ_RING = RING * OWN
MIXED = WIDTH_DEV + FEAT_RING
HIDDEN = 352
BOTH = 2 * HIDDEN

TN = (((0,), (0,)), ((), ()))
NT = (((1,), (1,)), ((), ()))


def in_vmem():
    return pl.BlockSpec(memory_space=pltpu.VMEM)


def anywhere():
    return pl.BlockSpec(memory_space=pl.ANY)


def shape(lengths, dtype):
    return jax.ShapeDtypeStruct(lengths, dtype)


def kernel(body, outs, in_specs, limit=12):
    single = not isinstance(outs, (list, tuple))
    return pl.pallas_call(
        body,
        out_shape=outs,
        in_specs=in_specs,
        out_specs=in_vmem() if single else [in_vmem() for _ in outs],
        compiler_params=pltpu.CompilerParams(vmem_limit_bytes=limit * 1024 * 1024),
    )


def silu(value):
    return value / (1.0 + jnp.exp(-value))


def high_low(value):
    high = value.astype(bf16).astype(f32)
    return high, value - high


def dot(left, right, dims=(((1,), (0,)), ((), ()))):
    return lax.dot_general(left, right, dims, preferred_element_type=f32)


def half_turn(value):
    return pltpu.roll(value, 64, 1)


def project(
    own_ref, gain_ref, gain_mid_ref, wq_ref, wk_ref, wv_ref, wg_ref, wb_ref, wd_ref, other_ref, after_ref, out_ref
):
    del after_ref
    on_first = lax.axis_index("tp") == 0
    own = own_ref[...].astype(f32)
    other = other_ref[...].astype(f32)
    rows = jnp.concatenate(
        [jnp.where(on_first, own, other), jnp.where(on_first, other, own)], axis=0
    ).T
    out_ref[:, TOKENS_AT:] = rows.astype(bf16)
    normed = (rows * gain_ref[...].astype(f32)).astype(bf16)
    for at, ref in enumerate((wq_ref, wk_ref, wv_ref, wg_ref)):
        out_ref[:, at * WIDTH_DEV : (at + 1) * WIDTH_DEV] = dot(normed, ref[...]).astype(bf16)
    beta = wb_ref[...].astype(f32)
    decay = wd_ref[...].astype(f32)
    small = jnp.concatenate(
        [
            jnp.where(on_first, beta[:HEADS_DEV], beta[HEADS_DEV:]),
            jnp.where(on_first, decay[:HEADS_DEV], decay[HEADS_DEV:]),
            jnp.zeros((128 - 2 * HEADS_DEV, 128), f32),
        ],
        axis=0,
    ).astype(bf16)
    extra = dot(normed, small, NT)
    lane = lax.broadcasted_iota(jnp.int32, extra.shape, 1)
    gain_mid = jnp.broadcast_to(gain_mid_ref[...].astype(f32), extra.shape)
    gain_mid = jnp.where(on_first, half_turn(gain_mid), gain_mid)
    out_ref[:, SMALL_AT:TOKENS_AT] = jnp.where(lane >= 64, gain_mid, extra).astype(bf16)


def pack(own_ref, other_ref, out_ref):
    on_first = lax.axis_index("tp") == 0
    own = own_ref[...].astype(f32)
    other = other_ref[...].astype(f32)
    low = lax.broadcasted_iota(jnp.int32, own.shape, 1) < 64
    top = jnp.where(on_first, own, half_turn(other))
    bottom = jnp.where(on_first, half_turn(other), own)
    out_ref[...] = jnp.where(low, top, bottom).astype(bf16)


def mixer(
    pieces_ref,
    state_ref,
    rate_ref,
    head_gain_ref,
    mixed_ref,
    key_ref,
    correct_ref,
    keep_ref,
    gain_ref,
):
    def total(first, last):
        parts = [pieces_ref[OWN * s : OWN * (s + 1), first:last].astype(f32) for s in range(GROUP)]
        while len(parts) > 1:
            parts = [a + b for a, b in zip(parts[::2], parts[1::2])]
        return parts[0]

    def block(s, at):
        return pieces_ref[OWN * s : OWN * (s + 1), at : at + 128].astype(f32)

    small = total(SMALL_AT, TOKENS_AT)
    tokens = [block(s, TOKENS_AT) for s in range(GROUP)]
    squares = sum(part * part for part in tokens)
    row_scale = lax.rsqrt(jnp.sum(squares, axis=1, keepdims=True) / D + norm_epsilon)
    small = small * row_scale
    row = lax.broadcasted_iota(jnp.int32, (OWN, HEAD_DIM), 0)
    lane = lax.broadcasted_iota(jnp.int32, (OWN, HEAD_DIM), 1)
    keeps = jnp.zeros((OWN, HEAD_DIM), f32)
    low = lane < 64
    for s in range(0, GROUP, 2):
        gain_ref[:, FEAT * s : FEAT * (s + 2)] = jnp.where(
            low, half_turn(block(s, SMALL_AT)), block(s + 1, SMALL_AT)
        )
        ring, at = s // RING, WIDTH_DEV + FEAT * (s % RING)
        first = jnp.where(low, tokens[s], half_turn(tokens[s + 1])).astype(bf16)
        second = jnp.where(low, half_turn(tokens[s]), tokens[s + 1]).astype(bf16)
        mixed_ref[OWN * 2 * ring : OWN * (2 * ring + 1), at : at + 128] = first
        mixed_ref[OWN * (2 * ring + 1) : OWN * (2 * ring + 2), at : at + 128] = second

    def unit(vector):
        return vector * lax.rsqrt(jnp.sum(vector * vector, axis=1, keepdims=True) + norm_epsilon)

    for h in range(HEADS_DEV):
        at = h * HEAD_DIM
        query_lin, key_lin, value_lin, gate_lin = (
            total(part * WIDTH_DEV + at, part * WIDTH_DEV + at + HEAD_DIM) * row_scale
            for part in range(4)
        )
        query = unit(silu(query_lin)) * HEAD_DIM ** (-0.5)
        key = unit(silu(key_lin))
        write_rate = 1.0 / (1.0 + jnp.exp(-small[:, h : h + 1]))
        decay = small[:, HEADS_DEV + h : HEADS_DEV + h + 1]
        softplus = jnp.maximum(decay, 0.0) + jnp.log1p(jnp.exp(-jnp.abs(decay)))
        keep = jnp.exp(-rate_ref[:, h : h + 1] * softplus)
        pair = jnp.concatenate([key, query], axis=0).astype(bf16)
        recalled = jnp.zeros((OWN, HEAD_DIM), f32)
        asked = jnp.zeros((OWN, HEAD_DIM), f32)
        for b in range(OWN):
            both = dot(pair, state_ref[b, h].astype(bf16))
            recalled = jnp.where(row == b, both[:OWN], recalled)
            asked = jnp.where(row == b, both[OWN:], asked)
        correction = write_rate * (silu(value_lin) - keep * recalled)
        readout = keep * asked + jnp.sum(key * query, axis=1, keepdims=True) * correction
        readout = readout * lax.rsqrt(
            jnp.mean(readout * readout, axis=1, keepdims=True) + norm_epsilon
        )
        mixed = (readout * head_gain_ref[...] * silu(gate_lin)).astype(bf16)
        for e in range(2 * RING):
            mixed_ref[OWN * e : OWN * (e + 1), at : at + HEAD_DIM] = mixed
        key_ref[:, at : at + HEAD_DIM] = key
        correct_ref[:, at : at + HEAD_DIM] = correction
        keeps = jnp.where(lane == h, keep, keeps)
    keep_ref[...] = keeps


def update(state_ref, key_ref, correct_ref, keep_ref, after_ref, next_ref, token_ref, made_ref, sems):
    del after_ref
    copies = []
    for b in range(OWN):
        for h in range(HEADS_DEV):
            at = h * HEAD_DIM
            key_column = jnp.broadcast_to(key_ref[b : b + 1, at : at + HEAD_DIM], (128, 128)).T
            made_ref[b, h] = (
                keep_ref[b : b + 1, h : h + 1] * state_ref[b, h]
                + key_column * correct_ref[b : b + 1, at : at + HEAD_DIM]
            )
        copies.append(pltpu.make_async_copy(made_ref.at[b], next_ref.at[b], sems.at[b]))
        copies[-1].start()
    token_ref[...] = jnp.zeros(token_ref.shape, f32)
    for copy in copies:
        copy.wait()


def updated(*operands):
    return pl.pallas_call(
        update,
        out_shape=[shape(operands[0].shape, f32), shape((8, 128), f32)],
        in_specs=[in_vmem()] * 4 + [anywhere()],
        out_specs=[pl.BlockSpec(memory_space=pltpu.HBM), in_vmem()],
        scratch_shapes=[
            pltpu.VMEM((OWN, HEADS_DEV, HEAD_DIM, HEAD_DIM), f32),
            pltpu.SemaphoreType.DMA((OWN,)),
        ],
        name="update",
        compiler_params=pltpu.CompilerParams(vmem_limit_bytes=12 * 1024 * 1024),
    )(*operands)


def preload(*refs):
    count = (len(refs) - 1) // 2
    sems = refs[-1]
    copies = [
        pltpu.make_async_copy(refs[i], refs[count + i], sems.at[i]) for i in range(count)
    ]
    for copy in copies:
        copy.start()
    for copy in copies:
        copy.wait()


def preloaded(*arrays):
    return pl.pallas_call(
        preload,
        out_shape=[shape(x.shape, x.dtype) for x in arrays],
        in_specs=[pl.BlockSpec(memory_space=pltpu.HBM)] * len(arrays),
        out_specs=[in_vmem() for _ in arrays],
        scratch_shapes=[pltpu.SemaphoreType.DMA((len(arrays),))],
        name="preload",
        compiler_params=pltpu.CompilerParams(vmem_limit_bytes=4 * 1024 * 1024),
    )(*(pltpu.with_memory_space_constraint(x, pltpu.HBM) for x in arrays))


def mix(received_ref, held_ref, next_ref, far_ref, last_ref, sent_ref):
    place = lax.axis_index("kv_1")

    def rows(core, first, last):
        return [
            received_ref[OWN * (2 * r + core) : OWN * (2 * r + core + 1), first:last].astype(f32)
            for r in range(RING)
        ]

    tokens = jnp.concatenate(rows(0, WIDTH_DEV, MIXED), axis=0)
    mixed = jnp.concatenate(rows(0, 0, WIDTH_DEV) + rows(1, 0, WIDTH_DEV), axis=0).astype(bf16)
    parts = []
    for ref in (held_ref, next_ref, far_ref, last_ref):
        both = dot(mixed, ref[...])
        parts.append(both[:SEQ_RING] + half_turn(both[SEQ_RING:]))

    def part(column):
        which = jnp.bitwise_xor(place, column)
        value = parts[0]
        for m in range(1, RING):
            value = jnp.where(which == m, parts[m], value)
        return value

    low = lax.broadcasted_iota(jnp.int32, parts[0].shape, 1) < 64
    attn = jnp.concatenate(
        [jnp.where(low, part(c), half_turn(part(c + 1))) for c in range(0, RING, 2)], axis=1
    )
    middle = (tokens + attn).astype(bf16)
    for s in range(GROUP):
        sent_ref[SEQ_RING * s : SEQ_RING * (s + 1)] = middle


def gate_up(received_ref, gain_ref, wg_ref, wu_ref, own_ref, sent_ref, middle_ref, rows_ref):
    for s in range(GROUP):
        ring, place = s // RING, s % RING
        for r in range(RING):
            rows_ref[
                SEQ_RING * r + OWN * place : SEQ_RING * r + OWN * (place + 1),
                FEAT_RING * ring : FEAT_RING * (ring + 1),
            ] = received_ref[SEQ_RING * s + OWN * r : SEQ_RING * s + OWN * (r + 1)]
    middle = rows_ref[...].astype(f32)
    normed = (middle * gain_ref[0:1]).astype(bf16)
    for at, ref in ((0, wg_ref), (HIDDEN, wu_ref)):
        value = dot(ref[...], normed, NT)
        own_ref[at : at + HIDDEN] = value
        sent_ref[at : at + HIDDEN] = value.astype(bf16)
    squares = jnp.sum(middle * middle, axis=1, keepdims=True)
    total = jnp.broadcast_to(squares, (ROWS, 128)).T[0:1]
    high, low = high_low(total)
    own_ref[BOTH:] = jnp.broadcast_to(total, (8, ROWS))
    sent_ref[BOTH:] = jnp.concatenate([high, low, jnp.zeros((6, ROWS), f32)], axis=0).astype(bf16)
    place = lax.axis_index("kv_1")
    pair = lax.axis_index("kv_0") * 2 + jnp.right_shift(place, 1)
    block = rows_ref[:, pl.ds(pl.multiple_of(pair * 128, 128), 128)].astype(f32).T
    even = jnp.bitwise_and(place, 1) == 0
    middle_ref[...] = jnp.where(even, block[:FEAT], block[FEAT:]).astype(bf16)


def down(own_ref, other_ref, w_ref, after_ref, out_ref):
    del after_ref
    squares = other_ref[BOTH:].astype(f32)
    total = own_ref[BOTH : BOTH + 1] + squares[0:1] + squares[1:2]
    scale = lax.rsqrt(total / D + norm_epsilon)
    gate = (own_ref[:HIDDEN] + other_ref[:HIDDEN].astype(f32)) * scale
    up = (own_ref[HIDDEN:BOTH] + other_ref[HIDDEN:BOTH].astype(f32)) * scale
    active = (silu(gate) * up).astype(bf16)
    out_ref[...] = dot(w_ref[...], active, TN).astype(bf16)


def finish(received_ref, middle_ref, out_ref):
    parts = [received_ref[FEAT * s : FEAT * (s + 1)].astype(f32) for s in range(GROUP)]
    while len(parts) > 1:
        parts = [a + b for a, b in zip(parts[::2], parts[1::2])]
    out_ref[...] = (middle_ref[...].astype(f32) + parts[0]).astype(bf16)


def from_other_core(array):
    return lax.ppermute(array, "tp", [(0, 1), (1, 0)])


def over(array, axes, members):
    tiles = array.reshape(members, array.shape[0] // members, array.shape[1])
    return lax.all_to_all(tiles, axes, 0, 0, tiled=True).reshape(array.shape)


def from_ring(array, flip):
    return lax.ppermute(array, "kv_1", [(i, i ^ flip) for i in range(RING)])


def layer(
    tokens,
    delta_state,
    gain_in,
    w_query,
    w_key,
    w_value,
    w_out_gate,
    w_beta,
    w_decay,
    decay_rate,
    head_gain,
    w_mix,
    gain_mid,
    w_gate,
    w_up,
    w_down,
):
    v, a = in_vmem(), anywhere()
    own_tokens = tokens.T
    other_tokens = from_other_core(own_tokens)
    other_mix = from_other_core(w_mix)
    *loaded, own_mix = preloaded(
        own_tokens,
        gain_in.reshape(1, 128),
        gain_mid.reshape(1, 128),
        w_query,
        w_key,
        w_value,
        w_out_gate,
        w_beta.T,
        w_decay.T,
        w_mix,
    )
    held = kernel(pack, shape(w_mix.shape, bf16), [v] * 2)(own_mix, other_mix)
    near = from_ring(held, 1)
    opposite = from_ring(held, 2)
    far = from_ring(held, 3)
    summand = kernel(project, shape((ROWS, PIECE), bf16), [v] * 10 + [a])(
        *loaded, other_tokens, held
    )
    pieces = over(summand, KV, GROUP)
    mixed, key, correction, keep, gains = kernel(
        mixer,
        [
            shape((2 * RING * OWN, MIXED), bf16),
            shape((OWN, WIDTH_DEV), f32),
            shape((OWN, WIDTH_DEV), f32),
            shape((OWN, HEAD_DIM), f32),
            shape((OWN, GROUP * FEAT), f32),
        ],
        [v] * 4,
    )(pieces, delta_state, decay_rate.reshape(1, HEADS_DEV), head_gain.reshape(1, HEAD_DIM))
    mixed_rows = over(mixed, ("kv_0", "tp"), 2 * RING)
    sent = kernel(mix, shape((GROUP * SEQ_RING, FEAT_RING), bf16), [v] * 5)(
        mixed_rows, held, near, opposite, far
    )
    received = over(sent, KV, GROUP)
    own_sum, sent_sum, middle = pl.pallas_call(
        gate_up,
        out_shape=[
            shape((BOTH + 8, ROWS), f32),
            shape((BOTH + 8, ROWS), bf16),
            shape((FEAT, ROWS), bf16),
        ],
        in_specs=[v] * 4,
        out_specs=[v] * 3,
        scratch_shapes=[pltpu.VMEM((ROWS, GROUP * FEAT), bf16)],
        name="gate_up",
        compiler_params=pltpu.CompilerParams(vmem_limit_bytes=12 * 1024 * 1024),
    )(received, gains, w_gate.T, w_up.T)
    next_state, token = updated(delta_state, key, correction, keep, received)
    down_local = kernel(down, shape((GROUP * FEAT, ROWS), bf16), [v, v, v, a])(
        own_sum, from_other_core(sent_sum), w_down, token
    )
    layer_out = kernel(finish, shape((FEAT, ROWS), bf16), [v] * 2)(
        over(down_local, KV, GROUP), middle
    )
    return (layer_out.T, next_state)


def solution(mesh):
    split = Mesh(
        mesh.devices.reshape(mesh.shape["dp"], 4, 4, mesh.shape["tp"]), ("dp", "kv_0", "kv_1", "tp")
    )
    in_specs = (
        P("dp", KV_TP),
        P(DP_KV, "tp", None, None),
        P(KV),
        P(KV, "tp"),
        P(KV, "tp"),
        P(KV, "tp"),
        P(KV, "tp"),
        P(KV, None),
        P(KV, None),
        P("tp"),
        P(),
        P("tp", KV),
        P(KV),
        P("tp", KV),
        P("tp", KV),
        P(KV, "tp"),
    )
    out_specs = (P("dp", KV_TP), P(DP_KV, "tp", None, None))
    return jax.shard_map(layer, mesh=split, in_specs=in_specs, out_specs=out_specs, check_vma=False)
```

```python
import jax
import jax.numpy as jnp
from jax import lax
from jax.experimental import pallas as pl
from jax.experimental.pallas import tpu as pltpu
from jax.sharding import Mesh
from jax.sharding import PartitionSpec as P


D = 2048
HEAD_DIM = 128
KV = ("kv_0", "kv_1")
KV_TP = ("kv_0", "kv_1", "tp")
DP_KV = ("dp", "kv_0", "kv_1")

norm_epsilon = 1e-06
bf16 = jnp.bfloat16
f32 = jnp.float32

GROUP = 16
ROWS = 128
OWN = ROWS // GROUP
FEAT = 64
HEADS_DEV = 4
WIDTH_DEV = HEADS_DEV * HEAD_DIM
SMALL_AT = 4 * WIDTH_DEV
TOKENS_AT = SMALL_AT + 128
PIECE = TOKENS_AT + 128
RING = 4
FEAT_RING = RING * FEAT
SEQ_RING = RING * OWN
MIXED = WIDTH_DEV + FEAT_RING
HIDDEN = 352
BOTH = 2 * HIDDEN

TN = (((0,), (0,)), ((), ()))
NT = (((1,), (1,)), ((), ()))


def in_vmem():
    return pl.BlockSpec(memory_space=pltpu.VMEM)


def anywhere():
    return pl.BlockSpec(memory_space=pl.ANY)


def shape(lengths, dtype):
    return jax.ShapeDtypeStruct(lengths, dtype)


def kernel(body, outs, in_specs, limit=12):
    single = not isinstance(outs, (list, tuple))
    return pl.pallas_call(
        body,
        out_shape=outs,
        in_specs=in_specs,
        out_specs=in_vmem() if single else [in_vmem() for _ in outs],
        compiler_params=pltpu.CompilerParams(vmem_limit_bytes=limit * 1024 * 1024),
    )


def silu(value):
    return value / (1.0 + jnp.exp(-value))


def high_low(value):
    high = value.astype(bf16).astype(f32)
    return high, value - high


def dot(left, right, dims=(((1,), (0,)), ((), ()))):
    return lax.dot_general(left, right, dims, preferred_element_type=f32)


def half_turn(value):
    return pltpu.roll(value, 64, 1)


def project(
    own_ref, gain_ref, gain_mid_ref, wq_ref, wk_ref, wv_ref, wg_ref, wb_ref, wd_ref, other_ref, after_ref, out_ref
):
    del after_ref
    on_first = lax.axis_index("tp") == 0
    own = own_ref[...].astype(f32)
    other = other_ref[...].astype(f32)
    rows = jnp.concatenate(
        [jnp.where(on_first, own, other), jnp.where(on_first, other, own)], axis=0
    ).T
    out_ref[:, TOKENS_AT:] = rows.astype(bf16)
    normed = (rows * gain_ref[...].astype(f32)).astype(bf16)
    for at, ref in enumerate((wq_ref, wk_ref, wv_ref, wg_ref)):
        out_ref[:, at * WIDTH_DEV : (at + 1) * WIDTH_DEV] = dot(normed, ref[...]).astype(bf16)
    beta = wb_ref[...].astype(f32)
    decay = wd_ref[...].astype(f32)
    small = jnp.concatenate(
        [
            jnp.where(on_first, beta[:HEADS_DEV], beta[HEADS_DEV:]),
            jnp.where(on_first, decay[:HEADS_DEV], decay[HEADS_DEV:]),
            jnp.zeros((128 - 2 * HEADS_DEV, 128), f32),
        ],
        axis=0,
    ).astype(bf16)
    extra = dot(normed, small, NT)
    lane = lax.broadcasted_iota(jnp.int32, extra.shape, 1)
    gain_mid = jnp.broadcast_to(gain_mid_ref[...].astype(f32), extra.shape)
    gain_mid = jnp.where(on_first, half_turn(gain_mid), gain_mid)
    out_ref[:, SMALL_AT:TOKENS_AT] = jnp.where(lane >= 64, gain_mid, extra).astype(bf16)


def pack(own_ref, other_ref, out_ref):
    on_first = lax.axis_index("tp") == 0
    own = own_ref[...].astype(f32)
    other = other_ref[...].astype(f32)
    low = lax.broadcasted_iota(jnp.int32, own.shape, 1) < 64
    top = jnp.where(on_first, own, half_turn(other))
    bottom = jnp.where(on_first, half_turn(other), own)
    out_ref[...] = jnp.where(low, top, bottom).astype(bf16)


def mixer(
    pieces_ref,
    state_ref,
    rate_ref,
    head_gain_ref,
    mixed_ref,
    key_ref,
    correct_ref,
    keep_ref,
    gain_ref,
):
    def total(first, last):
        parts = [pieces_ref[OWN * s : OWN * (s + 1), first:last].astype(f32) for s in range(GROUP)]
        while len(parts) > 1:
            parts = [a + b for a, b in zip(parts[::2], parts[1::2])]
        return parts[0]

    def block(s, at):
        return pieces_ref[OWN * s : OWN * (s + 1), at : at + 128].astype(f32)

    small = total(SMALL_AT, TOKENS_AT)
    tokens = [block(s, TOKENS_AT) for s in range(GROUP)]
    squares = sum(part * part for part in tokens)
    row_scale = lax.rsqrt(jnp.sum(squares, axis=1, keepdims=True) / D + norm_epsilon)
    small = small * row_scale
    row = lax.broadcasted_iota(jnp.int32, (OWN, HEAD_DIM), 0)
    lane = lax.broadcasted_iota(jnp.int32, (OWN, HEAD_DIM), 1)
    keeps = jnp.zeros((OWN, HEAD_DIM), f32)
    low = lane < 64
    for s in range(0, GROUP, 2):
        gain_ref[:, FEAT * s : FEAT * (s + 2)] = jnp.where(
            low, half_turn(block(s, SMALL_AT)), block(s + 1, SMALL_AT)
        )
        ring, at = s // RING, WIDTH_DEV + FEAT * (s % RING)
        first = jnp.where(low, tokens[s], half_turn(tokens[s + 1])).astype(bf16)
        second = jnp.where(low, half_turn(tokens[s]), tokens[s + 1]).astype(bf16)
        mixed_ref[OWN * 2 * ring : OWN * (2 * ring + 1), at : at + 128] = first
        mixed_ref[OWN * (2 * ring + 1) : OWN * (2 * ring + 2), at : at + 128] = second

    def unit(vector):
        return vector * lax.rsqrt(jnp.sum(vector * vector, axis=1, keepdims=True) + norm_epsilon)

    for h in range(HEADS_DEV):
        at = h * HEAD_DIM
        query_lin, key_lin, value_lin, gate_lin = (
            total(part * WIDTH_DEV + at, part * WIDTH_DEV + at + HEAD_DIM) * row_scale
            for part in range(4)
        )
        query = unit(silu(query_lin)) * HEAD_DIM ** (-0.5)
        key = unit(silu(key_lin))
        write_rate = 1.0 / (1.0 + jnp.exp(-small[:, h : h + 1]))
        decay = small[:, HEADS_DEV + h : HEADS_DEV + h + 1]
        softplus = jnp.maximum(decay, 0.0) + jnp.log1p(jnp.exp(-jnp.abs(decay)))
        keep = jnp.exp(-rate_ref[:, h : h + 1] * softplus)
        pair = jnp.concatenate([key, query], axis=0).astype(bf16)
        recalled = jnp.zeros((OWN, HEAD_DIM), f32)
        asked = jnp.zeros((OWN, HEAD_DIM), f32)
        for b in range(OWN):
            both = dot(pair, state_ref[b, h].astype(bf16))
            recalled = jnp.where(row == b, both[:OWN], recalled)
            asked = jnp.where(row == b, both[OWN:], asked)
        correction = write_rate * (silu(value_lin) - keep * recalled)
        readout = keep * asked + jnp.sum(key * query, axis=1, keepdims=True) * correction
        readout = readout * lax.rsqrt(
            jnp.mean(readout * readout, axis=1, keepdims=True) + norm_epsilon
        )
        mixed = (readout * head_gain_ref[...] * silu(gate_lin)).astype(bf16)
        for e in range(2 * RING):
            mixed_ref[OWN * e : OWN * (e + 1), at : at + HEAD_DIM] = mixed
        key_ref[:, at : at + HEAD_DIM] = key
        correct_ref[:, at : at + HEAD_DIM] = correction
        keeps = jnp.where(lane == h, keep, keeps)
    keep_ref[...] = keeps


def update(state_ref, key_ref, correct_ref, keep_ref, after_ref, next_ref, token_ref, made_ref, sems):
    del after_ref
    copies = []
    for b in range(OWN):
        for h in range(HEADS_DEV):
            at = h * HEAD_DIM
            key_column = jnp.broadcast_to(key_ref[b : b + 1, at : at + HEAD_DIM], (128, 128)).T
            made_ref[b, h] = (
                keep_ref[b : b + 1, h : h + 1] * state_ref[b, h]
                + key_column * correct_ref[b : b + 1, at : at + HEAD_DIM]
            )
        copies.append(pltpu.make_async_copy(made_ref.at[b], next_ref.at[b], sems.at[b]))
        copies[-1].start()
    token_ref[...] = jnp.zeros(token_ref.shape, f32)
    for copy in copies:
        copy.wait()


def updated(*operands):
    return pl.pallas_call(
        update,
        out_shape=[shape(operands[0].shape, f32), shape((8, 128), f32)],
        in_specs=[in_vmem()] * 4 + [anywhere()],
        out_specs=[pl.BlockSpec(memory_space=pltpu.HBM), in_vmem()],
        scratch_shapes=[
            pltpu.VMEM((OWN, HEADS_DEV, HEAD_DIM, HEAD_DIM), f32),
            pltpu.SemaphoreType.DMA((OWN,)),
        ],
        name="update",
        compiler_params=pltpu.CompilerParams(vmem_limit_bytes=12 * 1024 * 1024),
    )(*operands)


def preload(*refs):
    count = (len(refs) - 1) // 2
    sems = refs[-1]
    copies = [
        pltpu.make_async_copy(refs[i], refs[count + i], sems.at[i]) for i in range(count)
    ]
    for copy in copies:
        copy.start()
    for copy in copies:
        copy.wait()


def preloaded(*arrays):
    return pl.pallas_call(
        preload,
        out_shape=[shape(x.shape, x.dtype) for x in arrays],
        in_specs=[pl.BlockSpec(memory_space=pltpu.HBM)] * len(arrays),
        out_specs=[in_vmem() for _ in arrays],
        scratch_shapes=[pltpu.SemaphoreType.DMA((len(arrays),))],
        name="preload",
        compiler_params=pltpu.CompilerParams(vmem_limit_bytes=4 * 1024 * 1024),
    )(*(pltpu.with_memory_space_constraint(x, pltpu.HBM) for x in arrays))


def note(after_ref, out_ref):
    del after_ref
    out_ref[...] = jnp.zeros(out_ref.shape, f32)


def join(held_ref, near_ref, after_ref, out_ref):
    del after_ref
    out_ref[:WIDTH_DEV] = held_ref[...]
    out_ref[WIDTH_DEV:] = near_ref[...]


def ring_rows(received_ref, core, first, last):
    return [
        received_ref[OWN * (2 * r + core) : OWN * (2 * r + core + 1), first:last].astype(f32)
        for r in range(RING)
    ]


def ring_parts(received_ref, joined_ref):
    mixed = jnp.concatenate(
        ring_rows(received_ref, 0, 0, WIDTH_DEV) + ring_rows(received_ref, 1, 0, WIDTH_DEV), axis=0
    ).astype(bf16)
    parts = []
    for at in (0, WIDTH_DEV):
        both = dot(mixed, joined_ref[at : at + WIDTH_DEV])
        parts.append(both[:SEQ_RING] + half_turn(both[SEQ_RING:]))
    return parts


def mix_near(received_ref, joined_ref, part_ref):
    own, third = ring_parts(received_ref, joined_ref)
    part_ref[:SEQ_RING] = own
    part_ref[SEQ_RING:] = third


def mix(received_ref, far_ref, part_ref, sent_ref):
    place = lax.axis_index("kv_1")
    tokens = jnp.concatenate(ring_rows(received_ref, 0, WIDTH_DEV, MIXED), axis=0)
    first, second = ring_parts(received_ref, far_ref)
    parts = [part_ref[:SEQ_RING], first, second, part_ref[SEQ_RING:]]

    def part(column):
        which = jnp.bitwise_xor(place, column)
        value = parts[0]
        for m in range(1, RING):
            value = jnp.where(which == m, parts[m], value)
        return value

    low = lax.broadcasted_iota(jnp.int32, parts[0].shape, 1) < 64
    attn = jnp.concatenate(
        [jnp.where(low, part(c), half_turn(part(c + 1))) for c in range(0, RING, 2)], axis=1
    )
    middle = (tokens + attn).astype(bf16)
    for s in range(GROUP):
        sent_ref[SEQ_RING * s : SEQ_RING * (s + 1)] = middle


def gate_up(received_ref, gain_ref, wg_ref, wu_ref, own_ref, sent_ref, middle_ref, rows_ref):
    for s in range(GROUP):
        ring, place = s // RING, s % RING
        for r in range(RING):
            rows_ref[
                SEQ_RING * r + OWN * place : SEQ_RING * r + OWN * (place + 1),
                FEAT_RING * ring : FEAT_RING * (ring + 1),
            ] = received_ref[SEQ_RING * s + OWN * r : SEQ_RING * s + OWN * (r + 1)]
    middle = rows_ref[...].astype(f32)
    normed = (middle * gain_ref[0:1]).astype(bf16)
    for at, ref in ((0, wg_ref), (HIDDEN, wu_ref)):
        value = dot(ref[...], normed, NT)
        own_ref[at : at + HIDDEN] = value
        sent_ref[at : at + HIDDEN] = value.astype(bf16)
    squares = jnp.sum(middle * middle, axis=1, keepdims=True)
    total = jnp.broadcast_to(squares, (ROWS, 128)).T[0:1]
    high, low = high_low(total)
    own_ref[BOTH:] = jnp.broadcast_to(total, (8, ROWS))
    sent_ref[BOTH:] = jnp.concatenate([high, low, jnp.zeros((6, ROWS), f32)], axis=0).astype(bf16)
    place = lax.axis_index("kv_1")
    pair = lax.axis_index("kv_0") * 2 + jnp.right_shift(place, 1)
    block = rows_ref[:, pl.ds(pl.multiple_of(pair * 128, 128), 128)].astype(f32).T
    even = jnp.bitwise_and(place, 1) == 0
    middle_ref[...] = jnp.where(even, block[:FEAT], block[FEAT:]).astype(bf16)


def down(own_ref, other_ref, w_ref, after_ref, out_ref):
    del after_ref
    squares = other_ref[BOTH:].astype(f32)
    total = own_ref[BOTH : BOTH + 1] + squares[0:1] + squares[1:2]
    scale = lax.rsqrt(total / D + norm_epsilon)
    gate = (own_ref[:HIDDEN] + other_ref[:HIDDEN].astype(f32)) * scale
    up = (own_ref[HIDDEN:BOTH] + other_ref[HIDDEN:BOTH].astype(f32)) * scale
    active = (silu(gate) * up).astype(bf16)
    out_ref[...] = dot(w_ref[...], active, TN).astype(bf16)


def finish(received_ref, middle_ref, out_ref):
    parts = [received_ref[FEAT * s : FEAT * (s + 1)].astype(f32) for s in range(GROUP)]
    while len(parts) > 1:
        parts = [a + b for a, b in zip(parts[::2], parts[1::2])]
    out_ref[...] = (middle_ref[...].astype(f32) + parts[0]).astype(bf16)


def from_other_core(array):
    return lax.ppermute(array, "tp", [(0, 1), (1, 0)])


def over(array, axes, members):
    tiles = array.reshape(members, array.shape[0] // members, array.shape[1])
    return lax.all_to_all(tiles, axes, 0, 0, tiled=True).reshape(array.shape)


def from_ring(array, flip):
    return lax.ppermute(array, "kv_1", [(i, i ^ flip) for i in range(RING)])


def layer(
    tokens,
    delta_state,
    gain_in,
    w_query,
    w_key,
    w_value,
    w_out_gate,
    w_beta,
    w_decay,
    decay_rate,
    head_gain,
    w_mix,
    gain_mid,
    w_gate,
    w_up,
    w_down,
):
    v, a = in_vmem(), anywhere()
    own_tokens = tokens.T
    other_tokens = from_other_core(own_tokens)
    other_mix = from_other_core(w_mix)
    *loaded, own_mix = preloaded(
        own_tokens,
        gain_in.reshape(1, 128),
        gain_mid.reshape(1, 128),
        w_query,
        w_key,
        w_value,
        w_out_gate,
        w_beta.T,
        w_decay.T,
        w_mix,
    )
    held = kernel(pack, shape(w_mix.shape, bf16), [v] * 2)(own_mix, other_mix)
    near = from_ring(held, 3)
    summand = kernel(project, shape((ROWS, PIECE), bf16), [v] * 10 + [a])(
        *loaded, other_tokens, held
    )
    pieces = over(summand, KV, GROUP)
    mark = kernel(note, shape((8, 128), f32), [a])(pieces)
    joined = kernel(join, shape((2 * WIDTH_DEV, 128), bf16), [v, v, a])(held, near, mark)
    far = from_ring(joined, 1)
    mixed, key, correction, keep, gains = kernel(
        mixer,
        [
            shape((2 * RING * OWN, MIXED), bf16),
            shape((OWN, WIDTH_DEV), f32),
            shape((OWN, WIDTH_DEV), f32),
            shape((OWN, HEAD_DIM), f32),
            shape((OWN, GROUP * FEAT), f32),
        ],
        [v] * 4,
    )(pieces, delta_state, decay_rate.reshape(1, HEADS_DEV), head_gain.reshape(1, HEAD_DIM))
    mixed_rows = over(mixed, ("kv_0", "tp"), 2 * RING)
    near_part = kernel(mix_near, shape((2 * SEQ_RING, 128), f32), [v] * 2)(mixed_rows, joined)
    sent = kernel(mix, shape((GROUP * SEQ_RING, FEAT_RING), bf16), [v] * 3)(
        mixed_rows, far, near_part
    )
    received = over(sent, KV, GROUP)
    own_sum, sent_sum, middle = pl.pallas_call(
        gate_up,
        out_shape=[
            shape((BOTH + 8, ROWS), f32),
            shape((BOTH + 8, ROWS), bf16),
            shape((FEAT, ROWS), bf16),
        ],
        in_specs=[v] * 4,
        out_specs=[v] * 3,
        scratch_shapes=[pltpu.VMEM((ROWS, GROUP * FEAT), bf16)],
        name="gate_up",
        compiler_params=pltpu.CompilerParams(vmem_limit_bytes=12 * 1024 * 1024),
    )(received, gains, w_gate.T, w_up.T)
    next_state, token = updated(delta_state, key, correction, keep, received)
    down_local = kernel(down, shape((GROUP * FEAT, ROWS), bf16), [v, v, v, a])(
        own_sum, from_other_core(sent_sum), w_down, token
    )
    layer_out = kernel(finish, shape((FEAT, ROWS), bf16), [v] * 2)(
        over(down_local, KV, GROUP), middle
    )
    return (layer_out.T, next_state)


def solution(mesh):
    split = Mesh(
        mesh.devices.reshape(mesh.shape["dp"], 4, 4, mesh.shape["tp"]), ("dp", "kv_0", "kv_1", "tp")
    )
    in_specs = (
        P("dp", KV_TP),
        P(DP_KV, "tp", None, None),
        P(KV),
        P(KV, "tp"),
        P(KV, "tp"),
        P(KV, "tp"),
        P(KV, "tp"),
        P(KV, None),
        P(KV, None),
        P("tp"),
        P(),
        P("tp", KV),
        P(KV),
        P("tp", KV),
        P("tp", KV),
        P(KV, "tp"),
    )
    out_specs = (P("dp", KV_TP), P(DP_KV, "tp", None, None))
    return jax.shard_map(layer, mesh=split, in_specs=in_specs, out_specs=out_specs, check_vma=False)
```

```python
import jax
import jax.numpy as jnp
from jax import lax
from jax.experimental import pallas as pl
from jax.experimental.pallas import tpu as pltpu
from jax.sharding import Mesh
from jax.sharding import PartitionSpec as P


D = 2048
HEAD_DIM = 128
KV = ("kv_0", "kv_1")
KV_TP = ("kv_0", "kv_1", "tp")
DP_KV = ("dp", "kv_0", "kv_1")

norm_epsilon = 1e-06
bf16 = jnp.bfloat16
f32 = jnp.float32

GROUP = 16
ROWS = 128
OWN = ROWS // GROUP
FEAT = 64
HEADS_DEV = 4
WIDTH_DEV = HEADS_DEV * HEAD_DIM
SMALL_AT = 4 * WIDTH_DEV
TOKENS_AT = SMALL_AT + 128
PIECE = TOKENS_AT + 128
RING = 4
FEAT_RING = RING * FEAT
SEQ_RING = RING * OWN
MIXED = WIDTH_DEV + FEAT_RING
HIDDEN = 352
BOTH = 2 * HIDDEN

TN = (((0,), (0,)), ((), ()))
NT = (((1,), (1,)), ((), ()))


def in_vmem():
    return pl.BlockSpec(memory_space=pltpu.VMEM)


def anywhere():
    return pl.BlockSpec(memory_space=pl.ANY)


def shape(lengths, dtype):
    return jax.ShapeDtypeStruct(lengths, dtype)


def kernel(body, outs, in_specs, limit=12):
    single = not isinstance(outs, (list, tuple))
    return pl.pallas_call(
        body,
        out_shape=outs,
        in_specs=in_specs,
        out_specs=in_vmem() if single else [in_vmem() for _ in outs],
        compiler_params=pltpu.CompilerParams(vmem_limit_bytes=limit * 1024 * 1024),
    )


def silu(value):
    return value / (1.0 + jnp.exp(-value))


def high_low(value):
    high = value.astype(bf16).astype(f32)
    return high, value - high


def dot(left, right, dims=(((1,), (0,)), ((), ()))):
    return lax.dot_general(left, right, dims, preferred_element_type=f32)


def half_turn(value):
    return pltpu.roll(value, 64, 1)


def project(
    own_ref, gain_ref, gain_mid_ref, wq_ref, wk_ref, wv_ref, wg_ref, wb_ref, wd_ref, other_ref, after_ref, out_ref
):
    del after_ref
    on_first = lax.axis_index("tp") == 0
    own = own_ref[...].astype(f32)
    other = other_ref[...].astype(f32)
    rows = jnp.concatenate(
        [jnp.where(on_first, own, other), jnp.where(on_first, other, own)], axis=0
    ).T
    out_ref[:, TOKENS_AT:] = rows.astype(bf16)
    normed = (rows * gain_ref[...].astype(f32)).astype(bf16)
    for at, ref in enumerate((wq_ref, wk_ref, wv_ref, wg_ref)):
        out_ref[:, at * WIDTH_DEV : (at + 1) * WIDTH_DEV] = dot(normed, ref[...]).astype(bf16)
    beta = wb_ref[...].astype(f32)
    decay = wd_ref[...].astype(f32)
    small = jnp.concatenate(
        [
            jnp.where(on_first, beta[:HEADS_DEV], beta[HEADS_DEV:]),
            jnp.where(on_first, decay[:HEADS_DEV], decay[HEADS_DEV:]),
            jnp.zeros((128 - 2 * HEADS_DEV, 128), f32),
        ],
        axis=0,
    ).astype(bf16)
    extra = dot(normed, small, NT)
    lane = lax.broadcasted_iota(jnp.int32, extra.shape, 1)
    gain_mid = jnp.broadcast_to(gain_mid_ref[...].astype(f32), extra.shape)
    gain_mid = jnp.where(on_first, half_turn(gain_mid), gain_mid)
    out_ref[:, SMALL_AT:TOKENS_AT] = jnp.where(lane >= 64, gain_mid, extra).astype(bf16)


def pack(own_ref, other_ref, out_ref):
    on_first = lax.axis_index("tp") == 0
    own = own_ref[...].astype(f32)
    other = other_ref[...].astype(f32)
    low = lax.broadcasted_iota(jnp.int32, own.shape, 1) < 64
    top = jnp.where(on_first, own, half_turn(other))
    bottom = jnp.where(on_first, half_turn(other), own)
    out_ref[...] = jnp.where(low, top, bottom).astype(bf16)


def mixer(
    pieces_ref,
    state_ref,
    rate_ref,
    head_gain_ref,
    mixed_ref,
    key_ref,
    correct_ref,
    keep_ref,
    gain_ref,
):
    def total(first, last):
        parts = [pieces_ref[OWN * s : OWN * (s + 1), first:last].astype(f32) for s in range(GROUP)]
        while len(parts) > 1:
            parts = [a + b for a, b in zip(parts[::2], parts[1::2])]
        return parts[0]

    def block(s, at):
        return pieces_ref[OWN * s : OWN * (s + 1), at : at + 128].astype(f32)

    small = total(SMALL_AT, TOKENS_AT)
    tokens = [block(s, TOKENS_AT) for s in range(GROUP)]
    squares = sum(part * part for part in tokens)
    row_scale = lax.rsqrt(jnp.sum(squares, axis=1, keepdims=True) / D + norm_epsilon)
    small = small * row_scale
    own = jnp.bitwise_and(lax.broadcasted_iota(jnp.int32, (2 * OWN, HEAD_DIM), 0), OWN - 1)
    lane = lax.broadcasted_iota(jnp.int32, (OWN, HEAD_DIM), 1)
    keeps = jnp.zeros((OWN, HEAD_DIM), f32)
    low = lane < 64
    for s in range(0, GROUP, 2):
        gain_ref[:, FEAT * s : FEAT * (s + 2)] = jnp.where(
            low, half_turn(block(s, SMALL_AT)), block(s + 1, SMALL_AT)
        )
        ring, at = s // RING, WIDTH_DEV + FEAT * (s % RING)
        first = jnp.where(low, tokens[s], half_turn(tokens[s + 1])).astype(bf16)
        second = jnp.where(low, half_turn(tokens[s]), tokens[s + 1]).astype(bf16)
        mixed_ref[OWN * 2 * ring : OWN * (2 * ring + 1), at : at + 128] = first
        mixed_ref[OWN * (2 * ring + 1) : OWN * (2 * ring + 2), at : at + 128] = second

    def unit(vector):
        return vector * lax.rsqrt(jnp.sum(vector * vector, axis=1, keepdims=True) + norm_epsilon)

    for h in range(HEADS_DEV):
        at = h * HEAD_DIM
        query_lin, key_lin, value_lin, gate_lin = (
            total(part * WIDTH_DEV + at, part * WIDTH_DEV + at + HEAD_DIM) * row_scale
            for part in range(4)
        )
        query = unit(silu(query_lin)) * HEAD_DIM ** (-0.5)
        key = unit(silu(key_lin))
        write_rate = 1.0 / (1.0 + jnp.exp(-small[:, h : h + 1]))
        decay = small[:, HEADS_DEV + h : HEADS_DEV + h + 1]
        softplus = jnp.maximum(decay, 0.0) + jnp.log1p(jnp.exp(-jnp.abs(decay)))
        keep = jnp.exp(-rate_ref[:, h : h + 1] * softplus)
        pair = jnp.concatenate([key, query], axis=0)
        spread = jnp.concatenate([jnp.where(own == b, pair, 0.0) for b in range(OWN)], axis=1)
        states = state_ref[:, h].reshape(OWN * HEAD_DIM, HEAD_DIM)
        both = dot(spread.astype(bf16), states.astype(bf16))
        recalled, asked = both[:OWN], both[OWN:]
        correction = write_rate * (silu(value_lin) - keep * recalled)
        readout = keep * asked + jnp.sum(key * query, axis=1, keepdims=True) * correction
        readout = readout * lax.rsqrt(
            jnp.mean(readout * readout, axis=1, keepdims=True) + norm_epsilon
        )
        mixed = (readout * head_gain_ref[...] * silu(gate_lin)).astype(bf16)
        for e in range(2 * RING):
            mixed_ref[OWN * e : OWN * (e + 1), at : at + HEAD_DIM] = mixed
        key_ref[:, at : at + HEAD_DIM] = key
        correct_ref[:, at : at + HEAD_DIM] = correction
        keeps = jnp.where(lane == h, keep, keeps)
    keep_ref[...] = keeps


def update(state_ref, key_ref, correct_ref, keep_ref, after_ref, next_ref, token_ref, made_ref, sems):
    del after_ref
    copies = []
    for b in range(OWN):
        for h in range(HEADS_DEV):
            at = h * HEAD_DIM
            key_column = jnp.broadcast_to(key_ref[b : b + 1, at : at + HEAD_DIM], (128, 128)).T
            made_ref[b, h] = (
                keep_ref[b : b + 1, h : h + 1] * state_ref[b, h]
                + key_column * correct_ref[b : b + 1, at : at + HEAD_DIM]
            )
        copies.append(pltpu.make_async_copy(made_ref.at[b], next_ref.at[b], sems.at[b]))
        copies[-1].start()
    token_ref[...] = jnp.zeros(token_ref.shape, f32)
    for copy in copies:
        copy.wait()


def updated(*operands):
    return pl.pallas_call(
        update,
        out_shape=[shape(operands[0].shape, f32), shape((8, 128), f32)],
        in_specs=[in_vmem()] * 4 + [anywhere()],
        out_specs=[pl.BlockSpec(memory_space=pltpu.HBM), in_vmem()],
        scratch_shapes=[
            pltpu.VMEM((OWN, HEADS_DEV, HEAD_DIM, HEAD_DIM), f32),
            pltpu.SemaphoreType.DMA((OWN,)),
        ],
        name="update",
        compiler_params=pltpu.CompilerParams(vmem_limit_bytes=12 * 1024 * 1024),
    )(*operands)


def preload(*refs):
    count = (len(refs) - 1) // 2
    sems = refs[-1]
    copies = [
        pltpu.make_async_copy(refs[i], refs[count + i], sems.at[i]) for i in range(count)
    ]
    for copy in copies:
        copy.start()
    for copy in copies:
        copy.wait()


def preloaded(*arrays):
    return pl.pallas_call(
        preload,
        out_shape=[shape(x.shape, x.dtype) for x in arrays],
        in_specs=[pl.BlockSpec(memory_space=pltpu.HBM)] * len(arrays),
        out_specs=[in_vmem() for _ in arrays],
        scratch_shapes=[pltpu.SemaphoreType.DMA((len(arrays),))],
        name="preload",
        compiler_params=pltpu.CompilerParams(vmem_limit_bytes=4 * 1024 * 1024),
    )(*(pltpu.with_memory_space_constraint(x, pltpu.HBM) for x in arrays))


def note(after_ref, out_ref):
    del after_ref
    out_ref[...] = jnp.zeros(out_ref.shape, f32)


def join(held_ref, near_ref, after_ref, out_ref):
    del after_ref
    out_ref[:WIDTH_DEV] = held_ref[...]
    out_ref[WIDTH_DEV:] = near_ref[...]


def ring_rows(received_ref, core, first, last):
    return [
        received_ref[OWN * (2 * r + core) : OWN * (2 * r + core + 1), first:last].astype(f32)
        for r in range(RING)
    ]


def ring_parts(received_ref, joined_ref):
    mixed = jnp.concatenate(
        ring_rows(received_ref, 0, 0, WIDTH_DEV) + ring_rows(received_ref, 1, 0, WIDTH_DEV), axis=0
    ).astype(bf16)
    parts = []
    for at in (0, WIDTH_DEV):
        both = dot(mixed, joined_ref[at : at + WIDTH_DEV])
        parts.append(both[:SEQ_RING] + half_turn(both[SEQ_RING:]))
    return parts


def mix(received_ref, joined_ref, far_ref, after_ref, sent_ref):
    del after_ref
    place = lax.axis_index("kv_1")
    tokens = jnp.concatenate(ring_rows(received_ref, 0, WIDTH_DEV, MIXED), axis=0)
    held, third = ring_parts(received_ref, joined_ref)
    first, second = ring_parts(received_ref, far_ref)
    parts = [held, first, second, third]

    def part(column):
        which = jnp.bitwise_xor(place, column)
        value = parts[0]
        for m in range(1, RING):
            value = jnp.where(which == m, parts[m], value)
        return value

    low = lax.broadcasted_iota(jnp.int32, parts[0].shape, 1) < 64
    attn = jnp.concatenate(
        [jnp.where(low, part(c), half_turn(part(c + 1))) for c in range(0, RING, 2)], axis=1
    )
    middle = (tokens + attn).astype(bf16)
    for s in range(GROUP):
        sent_ref[SEQ_RING * s : SEQ_RING * (s + 1)] = middle


def gate_up(received_ref, gain_ref, wg_ref, wu_ref, own_ref, sent_ref, middle_ref, rows_ref):
    for s in range(GROUP):
        ring, place = s // RING, s % RING
        for r in range(RING):
            rows_ref[
                SEQ_RING * r + OWN * place : SEQ_RING * r + OWN * (place + 1),
                FEAT_RING * ring : FEAT_RING * (ring + 1),
            ] = received_ref[SEQ_RING * s + OWN * r : SEQ_RING * s + OWN * (r + 1)]
    middle = rows_ref[...].astype(f32)
    normed = (middle * gain_ref[0:1]).astype(bf16)
    for at, ref in ((0, wg_ref), (HIDDEN, wu_ref)):
        value = dot(ref[...], normed, NT)
        own_ref[at : at + HIDDEN] = value
        sent_ref[at : at + HIDDEN] = value.astype(bf16)
    squares = jnp.sum(middle * middle, axis=1, keepdims=True)
    total = jnp.broadcast_to(squares, (ROWS, 128)).T[0:1]
    high, low = high_low(total)
    own_ref[BOTH:] = jnp.broadcast_to(total, (8, ROWS))
    sent_ref[BOTH:] = jnp.concatenate([high, low, jnp.zeros((6, ROWS), f32)], axis=0).astype(bf16)
    place = lax.axis_index("kv_1")
    pair = lax.axis_index("kv_0") * 2 + jnp.right_shift(place, 1)
    block = rows_ref[:, pl.ds(pl.multiple_of(pair * 128, 128), 128)].astype(f32).T
    even = jnp.bitwise_and(place, 1) == 0
    middle_ref[...] = jnp.where(even, block[:FEAT], block[FEAT:]).astype(bf16)


def down(own_ref, other_ref, w_ref, after_ref, out_ref):
    del after_ref
    squares = other_ref[BOTH:].astype(f32)
    total = own_ref[BOTH : BOTH + 1] + squares[0:1] + squares[1:2]
    scale = lax.rsqrt(total / D + norm_epsilon)
    gate = (own_ref[:HIDDEN] + other_ref[:HIDDEN].astype(f32)) * scale
    up = (own_ref[HIDDEN:BOTH] + other_ref[HIDDEN:BOTH].astype(f32)) * scale
    active = (silu(gate) * up).astype(bf16)
    out_ref[...] = dot(w_ref[...], active, TN).astype(bf16)


def finish(received_ref, middle_ref, out_ref):
    parts = [received_ref[FEAT * s : FEAT * (s + 1)].astype(f32) for s in range(GROUP)]
    while len(parts) > 1:
        parts = [a + b for a, b in zip(parts[::2], parts[1::2])]
    out_ref[...] = (middle_ref[...].astype(f32) + parts[0]).astype(bf16)


def from_other_core(array):
    return lax.ppermute(array, "tp", [(0, 1), (1, 0)])


def over(array, axes, members):
    tiles = array.reshape(members, array.shape[0] // members, array.shape[1])
    return lax.all_to_all(tiles, axes, 0, 0, tiled=True).reshape(array.shape)


def from_ring(array, flip):
    return lax.ppermute(array, "kv_1", [(i, i ^ flip) for i in range(RING)])


def layer(
    tokens,
    delta_state,
    gain_in,
    w_query,
    w_key,
    w_value,
    w_out_gate,
    w_beta,
    w_decay,
    decay_rate,
    head_gain,
    w_mix,
    gain_mid,
    w_gate,
    w_up,
    w_down,
):
    v, a = in_vmem(), anywhere()
    own_tokens = tokens.T
    other_tokens = from_other_core(own_tokens)
    other_mix = from_other_core(w_mix)
    *loaded, own_mix = preloaded(
        own_tokens,
        gain_in.reshape(1, 128),
        gain_mid.reshape(1, 128),
        w_query,
        w_key,
        w_value,
        w_out_gate,
        w_beta.T,
        w_decay.T,
        w_mix,
    )
    held = kernel(pack, shape(w_mix.shape, bf16), [v] * 2)(own_mix, other_mix)
    near = from_ring(held, 3)
    summand = kernel(project, shape((ROWS, PIECE), bf16), [v] * 10 + [a])(
        *loaded, other_tokens, held
    )
    pieces = over(summand, KV, GROUP)
    mark = kernel(note, shape((8, 128), f32), [a])(pieces)
    joined = kernel(join, shape((2 * WIDTH_DEV, 128), bf16), [v, v, a])(held, near, mark)
    far = from_ring(joined, 1)
    mixed, key, correction, keep, gains = kernel(
        mixer,
        [
            shape((2 * RING * OWN, MIXED), bf16),
            shape((OWN, WIDTH_DEV), f32),
            shape((OWN, WIDTH_DEV), f32),
            shape((OWN, HEAD_DIM), f32),
            shape((OWN, GROUP * FEAT), f32),
        ],
        [v] * 4,
    )(pieces, delta_state, decay_rate.reshape(1, HEADS_DEV), head_gain.reshape(1, HEAD_DIM))
    mixed_rows = over(mixed, ("kv_0", "tp"), 2 * RING)
    arrived = kernel(note, shape((8, 128), f32), [a])(mixed_rows)
    sent = kernel(mix, shape((GROUP * SEQ_RING, FEAT_RING), bf16), [v] * 3 + [a])(
        mixed_rows, joined, far, arrived
    )
    received = over(sent, KV, GROUP)
    own_sum, sent_sum, middle = pl.pallas_call(
        gate_up,
        out_shape=[
            shape((BOTH + 8, ROWS), f32),
            shape((BOTH + 8, ROWS), bf16),
            shape((FEAT, ROWS), bf16),
        ],
        in_specs=[v] * 4,
        out_specs=[v] * 3,
        scratch_shapes=[pltpu.VMEM((ROWS, GROUP * FEAT), bf16)],
        name="gate_up",
        compiler_params=pltpu.CompilerParams(vmem_limit_bytes=12 * 1024 * 1024),
    )(received, gains, w_gate.T, w_up.T)
    next_state, token = updated(delta_state, key, correction, keep, received)
    down_local = kernel(down, shape((GROUP * FEAT, ROWS), bf16), [v, v, v, a])(
        own_sum, from_other_core(sent_sum), w_down, token
    )
    layer_out = kernel(finish, shape((FEAT, ROWS), bf16), [v] * 2)(
        over(down_local, KV, GROUP), middle
    )
    return (layer_out.T, next_state)


def solution(mesh):
    split = Mesh(
        mesh.devices.reshape(mesh.shape["dp"], 4, 4, mesh.shape["tp"]), ("dp", "kv_0", "kv_1", "tp")
    )
    in_specs = (
        P("dp", KV_TP),
        P(DP_KV, "tp", None, None),
        P(KV),
        P(KV, "tp"),
        P(KV, "tp"),
        P(KV, "tp"),
        P(KV, "tp"),
        P(KV, None),
        P(KV, None),
        P("tp"),
        P(),
        P("tp", KV),
        P(KV),
        P("tp", KV),
        P("tp", KV),
        P(KV, "tp"),
    )
    out_specs = (P("dp", KV_TP), P(DP_KV, "tp", None, None))
    return jax.shard_map(layer, mesh=split, in_specs=in_specs, out_specs=out_specs, check_vma=False)
```

```python
import jax
import jax.numpy as jnp
from jax import lax
from jax.experimental import pallas as pl
from jax.experimental.pallas import tpu as pltpu
from jax.sharding import Mesh
from jax.sharding import PartitionSpec as P


D = 2048
HEAD_DIM = 128
KV = ("kv_0", "kv_1")
KV_TP = ("kv_0", "kv_1", "tp")
DP_KV = ("dp", "kv_0", "kv_1")

norm_epsilon = 1e-06
bf16 = jnp.bfloat16
f32 = jnp.float32

GROUP = 16
ROWS = 128
OWN = ROWS // GROUP
FEAT = 64
HEADS_DEV = 4
WIDTH_DEV = HEADS_DEV * HEAD_DIM
SMALL_AT = 4 * WIDTH_DEV
PIECE = SMALL_AT + 128
RING = 4
FEAT_RING = RING * FEAT
SEQ_RING = RING * OWN
PACKED = WIDTH_DEV + SEQ_RING
JOINED = 2 * WIDTH_DEV + SEQ_RING
HIDDEN = 352
BOTH = 2 * HIDDEN

TN = (((0,), (0,)), ((), ()))
NT = (((1,), (1,)), ((), ()))


def in_vmem():
    return pl.BlockSpec(memory_space=pltpu.VMEM)


def anywhere():
    return pl.BlockSpec(memory_space=pl.ANY)


def shape(lengths, dtype):
    return jax.ShapeDtypeStruct(lengths, dtype)


def kernel(body, outs, in_specs, limit=12):
    single = not isinstance(outs, (list, tuple))
    return pl.pallas_call(
        body,
        out_shape=outs,
        in_specs=in_specs,
        out_specs=in_vmem() if single else [in_vmem() for _ in outs],
        compiler_params=pltpu.CompilerParams(vmem_limit_bytes=limit * 1024 * 1024),
    )


def silu(value):
    return value / (1.0 + jnp.exp(-value))


def high_low(value):
    high = value.astype(bf16).astype(f32)
    return high, value - high


def dot(left, right, dims=(((1,), (0,)), ((), ()))):
    return lax.dot_general(left, right, dims, preferred_element_type=f32)


def half_turn(value):
    return pltpu.roll(value, 64, 1)


def project(
    own_ref, gain_ref, gain_mid_ref, wq_ref, wk_ref, wv_ref, wg_ref, wb_ref, wd_ref, other_ref, out_ref, rows_ref
):
    on_first = lax.axis_index("tp") == 0
    own = own_ref[...].astype(f32)
    other = other_ref[...].astype(f32)
    rows = jnp.concatenate(
        [jnp.where(on_first, own, other), jnp.where(on_first, other, own)], axis=0
    ).T
    rows_ref[...] = rows.astype(bf16)
    high, low = high_low(jnp.sum(rows * rows, axis=1, keepdims=True))
    normed = (rows * gain_ref[...].astype(f32)).astype(bf16)
    for at, ref in enumerate((wq_ref, wk_ref, wv_ref, wg_ref)):
        out_ref[:, at * WIDTH_DEV : (at + 1) * WIDTH_DEV] = dot(normed, ref[...]).astype(bf16)
    beta = wb_ref[...].astype(f32)
    decay = wd_ref[...].astype(f32)
    small = jnp.concatenate(
        [
            jnp.where(on_first, beta[:HEADS_DEV], beta[HEADS_DEV:]),
            jnp.where(on_first, decay[:HEADS_DEV], decay[HEADS_DEV:]),
            jnp.zeros((128 - 2 * HEADS_DEV, 128), f32),
        ],
        axis=0,
    ).astype(bf16)
    extra = dot(normed, small, NT)
    lane = lax.broadcasted_iota(jnp.int32, extra.shape, 1)
    gain_mid = jnp.broadcast_to(gain_mid_ref[...].astype(f32), extra.shape)
    gain_mid = jnp.where(on_first, half_turn(gain_mid), gain_mid)
    extra = jnp.where(lane == 2 * HEADS_DEV, high, extra)
    extra = jnp.where(lane == 2 * HEADS_DEV + 1, low, extra)
    out_ref[:, SMALL_AT:] = jnp.where(lane >= 64, gain_mid, extra).astype(bf16)


def low_lanes(value):
    return lax.broadcasted_iota(jnp.int32, value.shape, 1) < 64


def ring_tokens(rows_ref, place, on_first, low):
    parts = [
        rows_ref[pl.ds(pl.multiple_of(SEQ_RING * r + OWN * place, OWN), OWN)].astype(f32)
        for r in range(RING)
    ]
    value = jnp.concatenate(parts, axis=0)
    turned = half_turn(value)
    return jnp.where(on_first, value, turned) if low else jnp.where(on_first, turned, value)


def pack(own_ref, other_ref, rows_ref, out_ref):
    on_first = lax.axis_index("tp") == 0
    place = lax.axis_index("kv_1")
    own = own_ref[...].astype(f32)
    other = other_ref[...].astype(f32)
    top = jnp.where(on_first, own, half_turn(other))
    bottom = jnp.where(on_first, half_turn(other), own)
    out_ref[:WIDTH_DEV] = jnp.where(low_lanes(own), top, bottom).astype(bf16)
    first = ring_tokens(rows_ref, jnp.bitwise_xor(place, 3), on_first, True)
    second = ring_tokens(rows_ref, jnp.bitwise_xor(place, 2), on_first, False)
    out_ref[WIDTH_DEV:] = jnp.where(low_lanes(first), first, second).astype(bf16)


def mixer(
    pieces_ref,
    state_ref,
    rate_ref,
    head_gain_ref,
    mixed_ref,
    key_ref,
    correct_ref,
    keep_ref,
    gain_ref,
):
    def total(first, last):
        parts = [pieces_ref[OWN * s : OWN * (s + 1), first:last].astype(f32) for s in range(GROUP)]
        while len(parts) > 1:
            parts = [a + b for a, b in zip(parts[::2], parts[1::2])]
        return parts[0]

    def block(s, at):
        return pieces_ref[OWN * s : OWN * (s + 1), at : at + 128].astype(f32)

    small = total(SMALL_AT, PIECE)
    lane = lax.broadcasted_iota(jnp.int32, (OWN, HEAD_DIM), 1)
    squares = jnp.where((lane == 2 * HEADS_DEV) | (lane == 2 * HEADS_DEV + 1), small, 0.0)
    row_scale = lax.rsqrt(jnp.sum(squares, axis=1, keepdims=True) / D + norm_epsilon)
    small = small * row_scale
    own = jnp.bitwise_and(lax.broadcasted_iota(jnp.int32, (2 * OWN, HEAD_DIM), 0), OWN - 1)
    keeps = jnp.zeros((OWN, HEAD_DIM), f32)
    low = lane < 64
    for s in range(0, GROUP, 2):
        gain_ref[:, FEAT * s : FEAT * (s + 2)] = jnp.where(
            low, half_turn(block(s, SMALL_AT)), block(s + 1, SMALL_AT)
        )

    def unit(vector):
        return vector * lax.rsqrt(jnp.sum(vector * vector, axis=1, keepdims=True) + norm_epsilon)

    for h in range(HEADS_DEV):
        at = h * HEAD_DIM
        query_lin, key_lin, value_lin, gate_lin = (
            total(part * WIDTH_DEV + at, part * WIDTH_DEV + at + HEAD_DIM) * row_scale
            for part in range(4)
        )
        query = unit(silu(query_lin)) * HEAD_DIM ** (-0.5)
        key = unit(silu(key_lin))
        write_rate = 1.0 / (1.0 + jnp.exp(-small[:, h : h + 1]))
        decay = small[:, HEADS_DEV + h : HEADS_DEV + h + 1]
        softplus = jnp.maximum(decay, 0.0) + jnp.log1p(jnp.exp(-jnp.abs(decay)))
        keep = jnp.exp(-rate_ref[:, h : h + 1] * softplus)
        pair = jnp.concatenate([key, query], axis=0)
        spread = jnp.concatenate([jnp.where(own == b, pair, 0.0) for b in range(OWN)], axis=1)
        states = state_ref[:, h].reshape(OWN * HEAD_DIM, HEAD_DIM)
        both = dot(spread.astype(bf16), states.astype(bf16))
        recalled, asked = both[:OWN], both[OWN:]
        correction = write_rate * (silu(value_lin) - keep * recalled)
        readout = keep * asked + jnp.sum(key * query, axis=1, keepdims=True) * correction
        readout = readout * lax.rsqrt(
            jnp.mean(readout * readout, axis=1, keepdims=True) + norm_epsilon
        )
        mixed = (readout * head_gain_ref[...] * silu(gate_lin)).astype(bf16)
        for e in range(2 * RING):
            mixed_ref[OWN * e : OWN * (e + 1), at : at + HEAD_DIM] = mixed
        key_ref[:, at : at + HEAD_DIM] = key
        correct_ref[:, at : at + HEAD_DIM] = correction
        keeps = jnp.where(lane == h, keep, keeps)
    keep_ref[...] = keeps


def update(state_ref, key_ref, correct_ref, keep_ref, after_ref, next_ref, token_ref, made_ref, sems):
    del after_ref
    copies = []
    for b in range(OWN):
        for h in range(HEADS_DEV):
            at = h * HEAD_DIM
            key_column = jnp.broadcast_to(key_ref[b : b + 1, at : at + HEAD_DIM], (128, 128)).T
            made_ref[b, h] = (
                keep_ref[b : b + 1, h : h + 1] * state_ref[b, h]
                + key_column * correct_ref[b : b + 1, at : at + HEAD_DIM]
            )
        copies.append(pltpu.make_async_copy(made_ref.at[b], next_ref.at[b], sems.at[b]))
        copies[-1].start()
    token_ref[...] = jnp.zeros(token_ref.shape, f32)
    for copy in copies:
        copy.wait()


def updated(*operands):
    return pl.pallas_call(
        update,
        out_shape=[shape(operands[0].shape, f32), shape((8, 128), f32)],
        in_specs=[in_vmem()] * 4 + [anywhere()],
        out_specs=[pl.BlockSpec(memory_space=pltpu.HBM), in_vmem()],
        scratch_shapes=[
            pltpu.VMEM((OWN, HEADS_DEV, HEAD_DIM, HEAD_DIM), f32),
            pltpu.SemaphoreType.DMA((OWN,)),
        ],
        name="update",
        compiler_params=pltpu.CompilerParams(vmem_limit_bytes=12 * 1024 * 1024),
    )(*operands)


def preload(*refs):
    count = (len(refs) - 1) // 2
    sems = refs[-1]
    copies = [
        pltpu.make_async_copy(refs[i], refs[count + i], sems.at[i]) for i in range(count)
    ]
    for copy in copies:
        copy.start()
    for copy in copies:
        copy.wait()


def preloaded(*arrays):
    return pl.pallas_call(
        preload,
        out_shape=[shape(x.shape, x.dtype) for x in arrays],
        in_specs=[pl.BlockSpec(memory_space=pltpu.HBM)] * len(arrays),
        out_specs=[in_vmem() for _ in arrays],
        scratch_shapes=[pltpu.SemaphoreType.DMA((len(arrays),))],
        name="preload",
        compiler_params=pltpu.CompilerParams(vmem_limit_bytes=4 * 1024 * 1024),
    )(*(pltpu.with_memory_space_constraint(x, pltpu.HBM) for x in arrays))


def note(after_ref, out_ref):
    del after_ref
    out_ref[...] = jnp.zeros(out_ref.shape, f32)


def join(held_ref, near_ref, rows_ref, after_ref, out_ref):
    del after_ref
    on_first = lax.axis_index("tp") == 0
    place = lax.axis_index("kv_1")
    out_ref[:WIDTH_DEV] = held_ref[:WIDTH_DEV]
    out_ref[WIDTH_DEV : 2 * WIDTH_DEV] = near_ref[:WIDTH_DEV]
    first = ring_tokens(rows_ref, jnp.bitwise_xor(place, 1), on_first, True)
    second = near_ref[WIDTH_DEV:].astype(f32)
    out_ref[2 * WIDTH_DEV :] = jnp.where(low_lanes(first), first, second).astype(bf16)


def ring_parts(received_ref, joined_ref):
    mixed = jnp.concatenate(
        [
            received_ref[OWN * (2 * r + core) : OWN * (2 * r + core + 1)].astype(f32)
            for core in range(2)
            for r in range(RING)
        ],
        axis=0,
    ).astype(bf16)
    parts = []
    for at in (0, WIDTH_DEV):
        both = dot(mixed, joined_ref[at : at + WIDTH_DEV])
        parts.append(both[:SEQ_RING] + half_turn(both[SEQ_RING:]))
    return parts


def mix(received_ref, joined_ref, near_ref, far_ref, rows_ref, after_ref, sent_ref):
    del after_ref
    on_first = lax.axis_index("tp") == 0
    place = lax.axis_index("kv_1")
    held, third = ring_parts(received_ref, joined_ref)
    first, second = ring_parts(received_ref, far_ref)
    far_tokens = far_ref[2 * WIDTH_DEV :].astype(f32)
    parts = [
        held + ring_tokens(rows_ref, place, on_first, True),
        first + far_tokens,
        second + half_turn(far_tokens),
        third + near_ref[WIDTH_DEV:].astype(f32),
    ]

    def part(column):
        which = jnp.bitwise_xor(place, column)
        value = parts[0]
        for m in range(1, RING):
            value = jnp.where(which == m, parts[m], value)
        return value

    low = low_lanes(parts[0])
    middle = jnp.concatenate(
        [jnp.where(low, part(c), half_turn(part(c + 1))) for c in range(0, RING, 2)], axis=1
    ).astype(bf16)
    for s in range(GROUP):
        sent_ref[SEQ_RING * s : SEQ_RING * (s + 1)] = middle


def gate_up(received_ref, gain_ref, wg_ref, wu_ref, own_ref, sent_ref, middle_ref, rows_ref):
    for s in range(GROUP):
        ring, place = s // RING, s % RING
        for r in range(RING):
            rows_ref[
                SEQ_RING * r + OWN * place : SEQ_RING * r + OWN * (place + 1),
                FEAT_RING * ring : FEAT_RING * (ring + 1),
            ] = received_ref[SEQ_RING * s + OWN * r : SEQ_RING * s + OWN * (r + 1)]
    middle = rows_ref[...].astype(f32)
    normed = (middle * gain_ref[0:1]).astype(bf16)
    for at, ref in ((0, wg_ref), (HIDDEN, wu_ref)):
        value = dot(ref[...], normed, NT)
        own_ref[at : at + HIDDEN] = value
        sent_ref[at : at + HIDDEN] = value.astype(bf16)
    squares = jnp.sum(middle * middle, axis=1, keepdims=True)
    total = jnp.broadcast_to(squares, (ROWS, 128)).T[0:1]
    high, low = high_low(total)
    own_ref[BOTH:] = jnp.broadcast_to(total, (8, ROWS))
    sent_ref[BOTH:] = jnp.concatenate([high, low, jnp.zeros((6, ROWS), f32)], axis=0).astype(bf16)
    place = lax.axis_index("kv_1")
    pair = lax.axis_index("kv_0") * 2 + jnp.right_shift(place, 1)
    block = rows_ref[:, pl.ds(pl.multiple_of(pair * 128, 128), 128)].astype(f32).T
    even = jnp.bitwise_and(place, 1) == 0
    middle_ref[...] = jnp.where(even, block[:FEAT], block[FEAT:]).astype(bf16)


def down(own_ref, other_ref, w_ref, after_ref, out_ref):
    del after_ref
    squares = other_ref[BOTH:].astype(f32)
    total = own_ref[BOTH : BOTH + 1] + squares[0:1] + squares[1:2]
    scale = lax.rsqrt(total / D + norm_epsilon)
    gate = (own_ref[:HIDDEN] + other_ref[:HIDDEN].astype(f32)) * scale
    up = (own_ref[HIDDEN:BOTH] + other_ref[HIDDEN:BOTH].astype(f32)) * scale
    active = (silu(gate) * up).astype(bf16)
    out_ref[...] = dot(w_ref[...], active, TN).astype(bf16)


def finish(received_ref, middle_ref, out_ref):
    parts = [received_ref[FEAT * s : FEAT * (s + 1)].astype(f32) for s in range(GROUP)]
    while len(parts) > 1:
        parts = [a + b for a, b in zip(parts[::2], parts[1::2])]
    out_ref[...] = (middle_ref[...].astype(f32) + parts[0]).astype(bf16)


def from_other_core(array):
    return lax.ppermute(array, "tp", [(0, 1), (1, 0)])


def over(array, axes, members):
    tiles = array.reshape(members, array.shape[0] // members, array.shape[1])
    return lax.all_to_all(tiles, axes, 0, 0, tiled=True).reshape(array.shape)


def from_ring(array, flip):
    return lax.ppermute(array, "kv_1", [(i, i ^ flip) for i in range(RING)])


def layer(
    tokens,
    delta_state,
    gain_in,
    w_query,
    w_key,
    w_value,
    w_out_gate,
    w_beta,
    w_decay,
    decay_rate,
    head_gain,
    w_mix,
    gain_mid,
    w_gate,
    w_up,
    w_down,
):
    v, a = in_vmem(), anywhere()
    own_tokens = tokens.T
    other_tokens = from_other_core(own_tokens)
    other_mix = from_other_core(w_mix)
    *loaded, own_mix = preloaded(
        own_tokens,
        gain_in.reshape(1, 128),
        gain_mid.reshape(1, 128),
        w_query,
        w_key,
        w_value,
        w_out_gate,
        w_beta.T,
        w_decay.T,
        w_mix,
    )
    summand, rows = kernel(
        project, [shape((ROWS, PIECE), bf16), shape((ROWS, 128), bf16)], [v] * 10
    )(*loaded, other_tokens)
    held = kernel(pack, shape((PACKED, 128), bf16), [v] * 3)(own_mix, other_mix, rows)
    near = from_ring(held, 3)
    pieces = over(summand, KV, GROUP)
    mark = kernel(note, shape((8, 128), f32), [a])(pieces)
    joined = kernel(join, shape((JOINED, 128), bf16), [v] * 3 + [a])(
        held, near, rows, mark
    )
    far = from_ring(joined, 1)
    mixed, key, correction, keep, gains = kernel(
        mixer,
        [
            shape((2 * RING * OWN, WIDTH_DEV), bf16),
            shape((OWN, WIDTH_DEV), f32),
            shape((OWN, WIDTH_DEV), f32),
            shape((OWN, HEAD_DIM), f32),
            shape((OWN, GROUP * FEAT), f32),
        ],
        [v] * 4,
    )(pieces, delta_state, decay_rate.reshape(1, HEADS_DEV), head_gain.reshape(1, HEAD_DIM))
    mixed_rows = over(mixed, ("kv_0", "tp"), 2 * RING)
    arrived = kernel(note, shape((8, 128), f32), [a])(mixed_rows)
    sent = kernel(mix, shape((GROUP * SEQ_RING, FEAT_RING), bf16), [v] * 5 + [a])(
        mixed_rows, joined, near, far, rows, arrived
    )
    received = over(sent, KV, GROUP)
    own_sum, sent_sum, middle = pl.pallas_call(
        gate_up,
        out_shape=[
            shape((BOTH + 8, ROWS), f32),
            shape((BOTH + 8, ROWS), bf16),
            shape((FEAT, ROWS), bf16),
        ],
        in_specs=[v] * 4,
        out_specs=[v] * 3,
        scratch_shapes=[pltpu.VMEM((ROWS, GROUP * FEAT), bf16)],
        name="gate_up",
        compiler_params=pltpu.CompilerParams(vmem_limit_bytes=12 * 1024 * 1024),
    )(received, gains, w_gate.T, w_up.T)
    next_state, token = updated(delta_state, key, correction, keep, received)
    down_local = kernel(down, shape((GROUP * FEAT, ROWS), bf16), [v, v, v, a])(
        own_sum, from_other_core(sent_sum), w_down, token
    )
    layer_out = kernel(finish, shape((FEAT, ROWS), bf16), [v] * 2)(
        over(down_local, KV, GROUP), middle
    )
    return (layer_out.T, next_state)


def solution(mesh):
    split = Mesh(
        mesh.devices.reshape(mesh.shape["dp"], 4, 4, mesh.shape["tp"]), ("dp", "kv_0", "kv_1", "tp")
    )
    in_specs = (
        P("dp", KV_TP),
        P(DP_KV, "tp", None, None),
        P(KV),
        P(KV, "tp"),
        P(KV, "tp"),
        P(KV, "tp"),
        P(KV, "tp"),
        P(KV, None),
        P(KV, None),
        P("tp"),
        P(),
        P("tp", KV),
        P(KV),
        P("tp", KV),
        P("tp", KV),
        P(KV, "tp"),
    )
    out_specs = (P("dp", KV_TP), P(DP_KV, "tp", None, None))
    return jax.shard_map(layer, mesh=split, in_specs=in_specs, out_specs=out_specs, check_vma=False)
```

```python
import jax
import jax.numpy as jnp
from jax import lax
from jax.experimental import pallas as pl
from jax.experimental.pallas import tpu as pltpu
from jax.sharding import Mesh
from jax.sharding import PartitionSpec as P


D = 2048
HEAD_DIM = 128
KV = ("kv_0", "kv_1")
KV_TP = ("kv_0", "kv_1", "tp")
DP_KV = ("dp", "kv_0", "kv_1")

norm_epsilon = 1e-06
bf16 = jnp.bfloat16
f32 = jnp.float32

GROUP = 16
ROWS = 128
OWN = ROWS // GROUP
FEAT = 64
HEADS_DEV = 4
WIDTH_DEV = HEADS_DEV * HEAD_DIM
SMALL_AT = 4 * WIDTH_DEV
PIECE = SMALL_AT + 128
RING = 4
FEAT_RING = RING * FEAT
SEQ_RING = RING * OWN
PACKED = WIDTH_DEV + SEQ_RING
JOINED = 2 * WIDTH_DEV + SEQ_RING
HIDDEN = 352
BOTH = 2 * HIDDEN

TN = (((0,), (0,)), ((), ()))
NT = (((1,), (1,)), ((), ()))


def in_vmem():
    return pl.BlockSpec(memory_space=pltpu.VMEM)


def anywhere():
    return pl.BlockSpec(memory_space=pl.ANY)


def shape(lengths, dtype):
    return jax.ShapeDtypeStruct(lengths, dtype)


def kernel(body, outs, in_specs, limit=12):
    single = not isinstance(outs, (list, tuple))
    return pl.pallas_call(
        body,
        out_shape=outs,
        in_specs=in_specs,
        out_specs=in_vmem() if single else [in_vmem() for _ in outs],
        compiler_params=pltpu.CompilerParams(vmem_limit_bytes=limit * 1024 * 1024),
    )


def silu(value):
    return value / (1.0 + jnp.exp(-value))


def high_low(value):
    high = value.astype(bf16).astype(f32)
    return high, value - high


def dot(left, right, dims=(((1,), (0,)), ((), ()))):
    return lax.dot_general(left, right, dims, preferred_element_type=f32)


def half_turn(value):
    return pltpu.roll(value, 64, 1)


def project(
    own_ref, gain_ref, gain_mid_ref, wq_ref, wk_ref, wv_ref, wg_ref, wb_ref, wd_ref, own_mix_ref, other_ref, other_mix_ref, out_ref, rows_ref, held_ref
):
    on_first = lax.axis_index("tp") == 0
    own = own_ref[...].astype(f32)
    other = other_ref[...].astype(f32)
    rows = jnp.concatenate(
        [jnp.where(on_first, own, other), jnp.where(on_first, other, own)], axis=0
    ).T
    rows_ref[...] = rows.astype(bf16)
    high, low = high_low(jnp.sum(rows * rows, axis=1, keepdims=True))
    normed = (rows * gain_ref[...].astype(f32)).astype(bf16)
    for at, ref in enumerate((wq_ref, wk_ref, wv_ref, wg_ref)):
        out_ref[:, at * WIDTH_DEV : (at + 1) * WIDTH_DEV] = dot(normed, ref[...]).astype(bf16)
    beta = wb_ref[...].astype(f32)
    decay = wd_ref[...].astype(f32)
    small = jnp.concatenate(
        [
            jnp.where(on_first, beta[:HEADS_DEV], beta[HEADS_DEV:]),
            jnp.where(on_first, decay[:HEADS_DEV], decay[HEADS_DEV:]),
            jnp.zeros((128 - 2 * HEADS_DEV, 128), f32),
        ],
        axis=0,
    ).astype(bf16)
    extra = dot(normed, small, NT)
    lane = lax.broadcasted_iota(jnp.int32, extra.shape, 1)
    gain_mid = jnp.broadcast_to(gain_mid_ref[...].astype(f32), extra.shape)
    gain_mid = jnp.where(on_first, half_turn(gain_mid), gain_mid)
    extra = jnp.where(lane == 2 * HEADS_DEV, high, extra)
    extra = jnp.where(lane == 2 * HEADS_DEV + 1, low, extra)
    out_ref[:, SMALL_AT:] = jnp.where(lane >= 64, gain_mid, extra).astype(bf16)
    pack(own_mix_ref, other_mix_ref, rows_ref, held_ref)


def low_lanes(value):
    return lax.broadcasted_iota(jnp.int32, value.shape, 1) < 64


def ring_tokens(rows_ref, place, on_first, low):
    parts = [
        rows_ref[pl.ds(pl.multiple_of(SEQ_RING * r + OWN * place, OWN), OWN)].astype(f32)
        for r in range(RING)
    ]
    value = jnp.concatenate(parts, axis=0)
    turned = half_turn(value)
    return jnp.where(on_first, value, turned) if low else jnp.where(on_first, turned, value)


def pack(own_ref, other_ref, rows_ref, out_ref):
    on_first = lax.axis_index("tp") == 0
    place = lax.axis_index("kv_1")
    own = own_ref[...].astype(f32)
    other = other_ref[...].astype(f32)
    top = jnp.where(on_first, own, half_turn(other))
    bottom = jnp.where(on_first, half_turn(other), own)
    out_ref[:WIDTH_DEV] = jnp.where(low_lanes(own), top, bottom).astype(bf16)
    first = ring_tokens(rows_ref, jnp.bitwise_xor(place, 3), on_first, True)
    second = ring_tokens(rows_ref, jnp.bitwise_xor(place, 2), on_first, False)
    out_ref[WIDTH_DEV:] = jnp.where(low_lanes(first), first, second).astype(bf16)


def mixer(
    pieces_ref,
    state_ref,
    rate_ref,
    head_gain_ref,
    mixed_ref,
    key_ref,
    correct_ref,
    keep_ref,
    gain_ref,
):
    def total(first, last):
        parts = [pieces_ref[OWN * s : OWN * (s + 1), first:last].astype(f32) for s in range(GROUP)]
        while len(parts) > 1:
            parts = [a + b for a, b in zip(parts[::2], parts[1::2])]
        return parts[0]

    def block(s, at):
        return pieces_ref[OWN * s : OWN * (s + 1), at : at + 128].astype(f32)

    small = total(SMALL_AT, PIECE)
    lane = lax.broadcasted_iota(jnp.int32, (OWN, HEAD_DIM), 1)
    squares = jnp.where((lane == 2 * HEADS_DEV) | (lane == 2 * HEADS_DEV + 1), small, 0.0)
    row_scale = lax.rsqrt(jnp.sum(squares, axis=1, keepdims=True) / D + norm_epsilon)
    small = small * row_scale
    own = jnp.bitwise_and(lax.broadcasted_iota(jnp.int32, (2 * OWN, HEAD_DIM), 0), OWN - 1)
    keeps = jnp.zeros((OWN, HEAD_DIM), f32)
    low = lane < 64
    for s in range(0, GROUP, 2):
        gain_ref[:, FEAT * s : FEAT * (s + 2)] = jnp.where(
            low, half_turn(block(s, SMALL_AT)), block(s + 1, SMALL_AT)
        )

    def unit(vector):
        return vector * lax.rsqrt(jnp.sum(vector * vector, axis=1, keepdims=True) + norm_epsilon)

    for h in range(HEADS_DEV):
        at = h * HEAD_DIM
        query_lin, key_lin, value_lin, gate_lin = (
            total(part * WIDTH_DEV + at, part * WIDTH_DEV + at + HEAD_DIM) * row_scale
            for part in range(4)
        )
        query = unit(silu(query_lin)) * HEAD_DIM ** (-0.5)
        key = unit(silu(key_lin))
        write_rate = 1.0 / (1.0 + jnp.exp(-small[:, h : h + 1]))
        decay = small[:, HEADS_DEV + h : HEADS_DEV + h + 1]
        softplus = jnp.maximum(decay, 0.0) + jnp.log1p(jnp.exp(-jnp.abs(decay)))
        keep = jnp.exp(-rate_ref[:, h : h + 1] * softplus)
        pair = jnp.concatenate([key, query], axis=0)
        spread = jnp.concatenate([jnp.where(own == b, pair, 0.0) for b in range(OWN)], axis=1)
        states = state_ref[:, h].reshape(OWN * HEAD_DIM, HEAD_DIM)
        both = dot(spread.astype(bf16), states.astype(bf16))
        recalled, asked = both[:OWN], both[OWN:]
        correction = write_rate * (silu(value_lin) - keep * recalled)
        readout = keep * asked + jnp.sum(key * query, axis=1, keepdims=True) * correction
        readout = readout * lax.rsqrt(
            jnp.mean(readout * readout, axis=1, keepdims=True) + norm_epsilon
        )
        mixed = (readout * head_gain_ref[...] * silu(gate_lin)).astype(bf16)
        for e in range(2 * RING):
            mixed_ref[OWN * e : OWN * (e + 1), at : at + HEAD_DIM] = mixed
        key_ref[:, at : at + HEAD_DIM] = key
        correct_ref[:, at : at + HEAD_DIM] = correction
        keeps = jnp.where(lane == h, keep, keeps)
    keep_ref[...] = keeps


def update(state_ref, key_ref, correct_ref, keep_ref, after_ref, next_ref, token_ref, made_ref, sems):
    del after_ref
    copies = []
    for b in range(OWN):
        for h in range(HEADS_DEV):
            at = h * HEAD_DIM
            key_column = jnp.broadcast_to(key_ref[b : b + 1, at : at + HEAD_DIM], (128, 128)).T
            made_ref[b, h] = (
                keep_ref[b : b + 1, h : h + 1] * state_ref[b, h]
                + key_column * correct_ref[b : b + 1, at : at + HEAD_DIM]
            )
        copies.append(pltpu.make_async_copy(made_ref.at[b], next_ref.at[b], sems.at[b]))
        copies[-1].start()
    token_ref[...] = jnp.zeros(token_ref.shape, f32)
    for copy in copies:
        copy.wait()


def updated(*operands):
    return pl.pallas_call(
        update,
        out_shape=[shape(operands[0].shape, f32), shape((8, 128), f32)],
        in_specs=[in_vmem()] * 4 + [anywhere()],
        out_specs=[pl.BlockSpec(memory_space=pltpu.HBM), in_vmem()],
        scratch_shapes=[
            pltpu.VMEM((OWN, HEADS_DEV, HEAD_DIM, HEAD_DIM), f32),
            pltpu.SemaphoreType.DMA((OWN,)),
        ],
        name="update",
        compiler_params=pltpu.CompilerParams(vmem_limit_bytes=12 * 1024 * 1024),
    )(*operands)


def preload(*refs):
    count = (len(refs) - 1) // 2
    sems = refs[-1]
    copies = [
        pltpu.make_async_copy(refs[i], refs[count + i], sems.at[i]) for i in range(count)
    ]
    for copy in copies:
        copy.start()
    for copy in copies:
        copy.wait()


def preloaded(*arrays):
    return pl.pallas_call(
        preload,
        out_shape=[shape(x.shape, x.dtype) for x in arrays],
        in_specs=[pl.BlockSpec(memory_space=pltpu.HBM)] * len(arrays),
        out_specs=[in_vmem() for _ in arrays],
        scratch_shapes=[pltpu.SemaphoreType.DMA((len(arrays),))],
        name="preload",
        compiler_params=pltpu.CompilerParams(vmem_limit_bytes=4 * 1024 * 1024),
    )(*(pltpu.with_memory_space_constraint(x, pltpu.HBM) for x in arrays))


def note(after_ref, out_ref):
    del after_ref
    out_ref[...] = jnp.zeros(out_ref.shape, f32)


def join(held_ref, near_ref, rows_ref, after_ref, out_ref):
    del after_ref
    on_first = lax.axis_index("tp") == 0
    place = lax.axis_index("kv_1")
    out_ref[:WIDTH_DEV] = held_ref[:WIDTH_DEV]
    out_ref[WIDTH_DEV : 2 * WIDTH_DEV] = near_ref[:WIDTH_DEV]
    first = ring_tokens(rows_ref, jnp.bitwise_xor(place, 1), on_first, True)
    second = near_ref[WIDTH_DEV:].astype(f32)
    out_ref[2 * WIDTH_DEV :] = jnp.where(low_lanes(first), first, second).astype(bf16)


def ring_parts(received_ref, joined_ref):
    mixed = jnp.concatenate(
        [
            received_ref[OWN * (2 * r + core) : OWN * (2 * r + core + 1)].astype(f32)
            for core in range(2)
            for r in range(RING)
        ],
        axis=0,
    ).astype(bf16)
    parts = []
    for at in (0, WIDTH_DEV):
        both = dot(mixed, joined_ref[at : at + WIDTH_DEV])
        parts.append(both[:SEQ_RING] + half_turn(both[SEQ_RING:]))
    return parts


def mix(received_ref, joined_ref, near_ref, far_ref, rows_ref, after_ref, sent_ref):
    del after_ref
    on_first = lax.axis_index("tp") == 0
    place = lax.axis_index("kv_1")
    held, third = ring_parts(received_ref, joined_ref)
    first, second = ring_parts(received_ref, far_ref)
    far_tokens = far_ref[2 * WIDTH_DEV :].astype(f32)
    parts = [
        held + ring_tokens(rows_ref, place, on_first, True),
        first + far_tokens,
        second + half_turn(far_tokens),
        third + near_ref[WIDTH_DEV:].astype(f32),
    ]

    def part(column):
        which = jnp.bitwise_xor(place, column)
        value = parts[0]
        for m in range(1, RING):
            value = jnp.where(which == m, parts[m], value)
        return value

    low = low_lanes(parts[0])
    middle = jnp.concatenate(
        [jnp.where(low, part(c), half_turn(part(c + 1))) for c in range(0, RING, 2)], axis=1
    ).astype(bf16)
    for s in range(GROUP):
        sent_ref[SEQ_RING * s : SEQ_RING * (s + 1)] = middle


def gate_up(received_ref, gain_ref, wg_ref, wu_ref, own_ref, sent_ref, middle_ref, rows_ref):
    for s in range(GROUP):
        ring, place = s // RING, s % RING
        for r in range(RING):
            rows_ref[
                SEQ_RING * r + OWN * place : SEQ_RING * r + OWN * (place + 1),
                FEAT_RING * ring : FEAT_RING * (ring + 1),
            ] = received_ref[SEQ_RING * s + OWN * r : SEQ_RING * s + OWN * (r + 1)]
    middle = rows_ref[...].astype(f32)
    normed = (middle * gain_ref[0:1]).astype(bf16)
    for at, ref in ((0, wg_ref), (HIDDEN, wu_ref)):
        value = dot(ref[...], normed, NT)
        own_ref[at : at + HIDDEN] = value
        sent_ref[at : at + HIDDEN] = value.astype(bf16)
    squares = jnp.sum(middle * middle, axis=1, keepdims=True)
    total = jnp.broadcast_to(squares, (ROWS, 128)).T[0:1]
    high, low = high_low(total)
    own_ref[BOTH:] = jnp.broadcast_to(total, (8, ROWS))
    sent_ref[BOTH:] = jnp.concatenate([high, low, jnp.zeros((6, ROWS), f32)], axis=0).astype(bf16)
    place = lax.axis_index("kv_1")
    pair = lax.axis_index("kv_0") * 2 + jnp.right_shift(place, 1)
    block = rows_ref[:, pl.ds(pl.multiple_of(pair * 128, 128), 128)].astype(f32).T
    even = jnp.bitwise_and(place, 1) == 0
    middle_ref[...] = jnp.where(even, block[:FEAT], block[FEAT:]).astype(bf16)


def down(own_ref, other_ref, w_ref, after_ref, out_ref):
    del after_ref
    squares = other_ref[BOTH:].astype(f32)
    total = own_ref[BOTH : BOTH + 1] + squares[0:1] + squares[1:2]
    scale = lax.rsqrt(total / D + norm_epsilon)
    gate = (own_ref[:HIDDEN] + other_ref[:HIDDEN].astype(f32)) * scale
    up = (own_ref[HIDDEN:BOTH] + other_ref[HIDDEN:BOTH].astype(f32)) * scale
    active = (silu(gate) * up).astype(bf16)
    out_ref[...] = dot(w_ref[...], active, TN).astype(bf16)


def finish(received_ref, middle_ref, out_ref):
    parts = [received_ref[FEAT * s : FEAT * (s + 1)].astype(f32) for s in range(GROUP)]
    while len(parts) > 1:
        parts = [a + b for a, b in zip(parts[::2], parts[1::2])]
    out_ref[...] = (middle_ref[...].astype(f32) + parts[0]).astype(bf16)


def from_other_core(array):
    return lax.ppermute(array, "tp", [(0, 1), (1, 0)])


def over(array, axes, members):
    tiles = array.reshape(members, array.shape[0] // members, array.shape[1])
    return lax.all_to_all(tiles, axes, 0, 0, tiled=True).reshape(array.shape)


def from_ring(array, flip):
    return lax.ppermute(array, "kv_1", [(i, i ^ flip) for i in range(RING)])


def layer(
    tokens,
    delta_state,
    gain_in,
    w_query,
    w_key,
    w_value,
    w_out_gate,
    w_beta,
    w_decay,
    decay_rate,
    head_gain,
    w_mix,
    gain_mid,
    w_gate,
    w_up,
    w_down,
):
    v, a = in_vmem(), anywhere()
    own_tokens = tokens.T
    other_tokens = from_other_core(own_tokens)
    other_mix = from_other_core(w_mix)
    loaded = preloaded(
        own_tokens,
        gain_in.reshape(1, 128),
        gain_mid.reshape(1, 128),
        w_query,
        w_key,
        w_value,
        w_out_gate,
        w_beta.T,
        w_decay.T,
        w_mix,
    )
    summand, rows, held = kernel(
        project,
        [shape((ROWS, PIECE), bf16), shape((ROWS, 128), bf16), shape((PACKED, 128), bf16)],
        [v] * 12,
    )(*loaded, other_tokens, other_mix)
    near = from_ring(held, 3)
    pieces = over(summand, KV, GROUP)
    mark = kernel(note, shape((8, 128), f32), [a])(pieces)
    joined = kernel(join, shape((JOINED, 128), bf16), [v] * 3 + [a])(
        held, near, rows, mark
    )
    far = from_ring(joined, 1)
    mixed, key, correction, keep, gains = kernel(
        mixer,
        [
            shape((2 * RING * OWN, WIDTH_DEV), bf16),
            shape((OWN, WIDTH_DEV), f32),
            shape((OWN, WIDTH_DEV), f32),
            shape((OWN, HEAD_DIM), f32),
            shape((OWN, GROUP * FEAT), f32),
        ],
        [v] * 4,
    )(pieces, delta_state, decay_rate.reshape(1, HEADS_DEV), head_gain.reshape(1, HEAD_DIM))
    mixed_rows = over(mixed, ("kv_0", "tp"), 2 * RING)
    arrived = kernel(note, shape((8, 128), f32), [a])(mixed_rows)
    sent = kernel(mix, shape((GROUP * SEQ_RING, FEAT_RING), bf16), [v] * 5 + [a])(
        mixed_rows, joined, near, far, rows, arrived
    )
    received = over(sent, KV, GROUP)
    own_sum, sent_sum, middle = pl.pallas_call(
        gate_up,
        out_shape=[
            shape((BOTH + 8, ROWS), f32),
            shape((BOTH + 8, ROWS), bf16),
            shape((FEAT, ROWS), bf16),
        ],
        in_specs=[v] * 4,
        out_specs=[v] * 3,
        scratch_shapes=[pltpu.VMEM((ROWS, GROUP * FEAT), bf16)],
        name="gate_up",
        compiler_params=pltpu.CompilerParams(vmem_limit_bytes=12 * 1024 * 1024),
    )(received, gains, w_gate.T, w_up.T)
    next_state, token = updated(delta_state, key, correction, keep, received)
    down_local = kernel(down, shape((GROUP * FEAT, ROWS), bf16), [v, v, v, a])(
        own_sum, from_other_core(sent_sum), w_down, token
    )
    layer_out = kernel(finish, shape((FEAT, ROWS), bf16), [v] * 2)(
        over(down_local, KV, GROUP), middle
    )
    return (layer_out.T, next_state)


def solution(mesh):
    split = Mesh(
        mesh.devices.reshape(mesh.shape["dp"], 4, 4, mesh.shape["tp"]), ("dp", "kv_0", "kv_1", "tp")
    )
    in_specs = (
        P("dp", KV_TP),
        P(DP_KV, "tp", None, None),
        P(KV),
        P(KV, "tp"),
        P(KV, "tp"),
        P(KV, "tp"),
        P(KV, "tp"),
        P(KV, None),
        P(KV, None),
        P("tp"),
        P(),
        P("tp", KV),
        P(KV),
        P("tp", KV),
        P("tp", KV),
        P(KV, "tp"),
    )
    out_specs = (P("dp", KV_TP), P(DP_KV, "tp", None, None))
    return jax.shard_map(layer, mesh=split, in_specs=in_specs, out_specs=out_specs, check_vma=False)
```

```python
import jax
import jax.numpy as jnp
from jax import lax
from jax.experimental import pallas as pl
from jax.experimental.pallas import tpu as pltpu
from jax.sharding import Mesh
from jax.sharding import PartitionSpec as P


D = 2048
HEAD_DIM = 128
KV = ("kv_0", "kv_1")
KV_TP = ("kv_0", "kv_1", "tp")
DP_KV = ("dp", "kv_0", "kv_1")

norm_epsilon = 1e-06
bf16 = jnp.bfloat16
f32 = jnp.float32

GROUP = 16
ROWS = 128
OWN = ROWS // GROUP
FEAT = 64
HEADS_DEV = 4
WIDTH_DEV = HEADS_DEV * HEAD_DIM
SMALL_AT = 4 * WIDTH_DEV
PIECE = SMALL_AT + 128
RING = 4
FEAT_RING = RING * FEAT
SEQ_RING = RING * OWN
PACKED = WIDTH_DEV + SEQ_RING
JOINED = 2 * WIDTH_DEV + SEQ_RING
HIDDEN = 352
BOTH = 2 * HIDDEN

TN = (((0,), (0,)), ((), ()))
NT = (((1,), (1,)), ((), ()))


def in_vmem():
    return pl.BlockSpec(memory_space=pltpu.VMEM)


def anywhere():
    return pl.BlockSpec(memory_space=pl.ANY)


def shape(lengths, dtype):
    return jax.ShapeDtypeStruct(lengths, dtype)


def kernel(body, outs, in_specs, limit=12):
    single = not isinstance(outs, (list, tuple))
    return pl.pallas_call(
        body,
        out_shape=outs,
        in_specs=in_specs,
        out_specs=in_vmem() if single else [in_vmem() for _ in outs],
        compiler_params=pltpu.CompilerParams(vmem_limit_bytes=limit * 1024 * 1024),
    )


def silu(value):
    return value / (1.0 + jnp.exp(-value))


def high_low(value):
    high = value.astype(bf16).astype(f32)
    return high, value - high


def dot(left, right, dims=(((1,), (0,)), ((), ()))):
    return lax.dot_general(left, right, dims, preferred_element_type=f32)


def half_turn(value):
    return pltpu.roll(value, 64, 1)


def project(
    own_ref, gain_ref, gain_mid_ref, wq_ref, wk_ref, wv_ref, wg_ref, wb_ref, wd_ref, own_mix_ref, other_ref, other_mix_ref, out_ref, rows_ref, held_ref
):
    on_first = lax.axis_index("tp") == 0
    own = own_ref[...].astype(f32)
    other = other_ref[...].astype(f32)
    rows = jnp.concatenate(
        [jnp.where(on_first, own, other), jnp.where(on_first, other, own)], axis=0
    ).T
    rows_ref[...] = rows.astype(bf16)
    high, low = high_low(jnp.sum(rows * rows, axis=1, keepdims=True))
    normed = (rows * gain_ref[...].astype(f32)).astype(bf16)
    for at, ref in enumerate((wq_ref, wk_ref, wv_ref, wg_ref)):
        out_ref[:, at * WIDTH_DEV : (at + 1) * WIDTH_DEV] = dot(normed, ref[...]).astype(bf16)
    beta = wb_ref[...].astype(f32)
    decay = wd_ref[...].astype(f32)
    small = jnp.concatenate(
        [
            jnp.where(on_first, beta[:HEADS_DEV], beta[HEADS_DEV:]),
            jnp.where(on_first, decay[:HEADS_DEV], decay[HEADS_DEV:]),
            jnp.zeros((128 - 2 * HEADS_DEV, 128), f32),
        ],
        axis=0,
    ).astype(bf16)
    extra = dot(normed, small, NT)
    lane = lax.broadcasted_iota(jnp.int32, extra.shape, 1)
    gain_mid = jnp.broadcast_to(gain_mid_ref[...].astype(f32), extra.shape)
    gain_mid = jnp.where(on_first, half_turn(gain_mid), gain_mid)
    extra = jnp.where(lane == 2 * HEADS_DEV, high, extra)
    extra = jnp.where(lane == 2 * HEADS_DEV + 1, low, extra)
    out_ref[:, SMALL_AT:] = jnp.where(lane >= 64, gain_mid, extra).astype(bf16)
    pack(own_mix_ref, other_mix_ref, rows_ref, held_ref)


def low_lanes(value):
    return lax.broadcasted_iota(jnp.int32, value.shape, 1) < 64


def ring_tokens(rows_ref, place, on_first, low):
    parts = [
        rows_ref[pl.ds(pl.multiple_of(SEQ_RING * r + OWN * place, OWN), OWN)].astype(f32)
        for r in range(RING)
    ]
    value = jnp.concatenate(parts, axis=0)
    turned = half_turn(value)
    return jnp.where(on_first, value, turned) if low else jnp.where(on_first, turned, value)


def pack(own_ref, other_ref, rows_ref, out_ref):
    on_first = lax.axis_index("tp") == 0
    place = lax.axis_index("kv_1")
    own = own_ref[...].astype(f32)
    other = other_ref[...].astype(f32)
    top = jnp.where(on_first, own, half_turn(other))
    bottom = jnp.where(on_first, half_turn(other), own)
    out_ref[:WIDTH_DEV] = jnp.where(low_lanes(own), top, bottom).astype(bf16)
    first = ring_tokens(rows_ref, jnp.bitwise_xor(place, 3), on_first, True)
    second = ring_tokens(rows_ref, jnp.bitwise_xor(place, 2), on_first, False)
    out_ref[WIDTH_DEV:] = jnp.where(low_lanes(first), first, second).astype(bf16)


def mixer(
    pieces_ref,
    state_ref,
    rate_ref,
    head_gain_ref,
    mixed_ref,
    key_ref,
    correct_ref,
    keep_ref,
    gain_ref,
):
    def total(first, last):
        parts = [pieces_ref[OWN * s : OWN * (s + 1), first:last].astype(f32) for s in range(GROUP)]
        while len(parts) > 1:
            parts = [a + b for a, b in zip(parts[::2], parts[1::2])]
        return parts[0]

    def block(s, at):
        return pieces_ref[OWN * s : OWN * (s + 1), at : at + 128].astype(f32)

    small = total(SMALL_AT, PIECE)
    lane = lax.broadcasted_iota(jnp.int32, (OWN, HEAD_DIM), 1)
    squares = jnp.where((lane == 2 * HEADS_DEV) | (lane == 2 * HEADS_DEV + 1), small, 0.0)
    row_scale = lax.rsqrt(jnp.sum(squares, axis=1, keepdims=True) / D + norm_epsilon)
    small = small * row_scale
    own = jnp.bitwise_and(lax.broadcasted_iota(jnp.int32, (2 * OWN, HEAD_DIM), 0), OWN - 1)
    keeps = jnp.zeros((OWN, HEAD_DIM), f32)
    low = lane < 64
    for s in range(0, GROUP, 2):
        gain_ref[:, FEAT * s : FEAT * (s + 2)] = jnp.where(
            low, half_turn(block(s, SMALL_AT)), block(s + 1, SMALL_AT)
        )

    def unit(vector):
        return vector * lax.rsqrt(jnp.sum(vector * vector, axis=1, keepdims=True) + norm_epsilon)

    for h in range(HEADS_DEV):
        at = h * HEAD_DIM
        query_lin, key_lin, value_lin, gate_lin = (
            total(part * WIDTH_DEV + at, part * WIDTH_DEV + at + HEAD_DIM) * row_scale
            for part in range(4)
        )
        query = unit(silu(query_lin)) * HEAD_DIM ** (-0.5)
        key = unit(silu(key_lin))
        write_rate = 1.0 / (1.0 + jnp.exp(-small[:, h : h + 1]))
        decay = small[:, HEADS_DEV + h : HEADS_DEV + h + 1]
        softplus = jnp.maximum(decay, 0.0) + jnp.log1p(jnp.exp(-jnp.abs(decay)))
        keep = jnp.exp(-rate_ref[:, h : h + 1] * softplus)
        pair = jnp.concatenate([key, query], axis=0)
        spread = jnp.concatenate([jnp.where(own == b, pair, 0.0) for b in range(OWN)], axis=1)
        states = state_ref[:, h].reshape(OWN * HEAD_DIM, HEAD_DIM)
        both = dot(spread.astype(bf16), states.astype(bf16))
        recalled, asked = both[:OWN], both[OWN:]
        correction = write_rate * (silu(value_lin) - keep * recalled)
        readout = keep * asked + jnp.sum(key * query, axis=1, keepdims=True) * correction
        readout = readout * lax.rsqrt(
            jnp.mean(readout * readout, axis=1, keepdims=True) + norm_epsilon
        )
        mixed = (readout * head_gain_ref[...] * silu(gate_lin)).astype(bf16)
        for e in range(2 * RING):
            mixed_ref[OWN * e : OWN * (e + 1), at : at + HEAD_DIM] = mixed
        key_ref[:, at : at + HEAD_DIM] = key
        correct_ref[:, at : at + HEAD_DIM] = correction
        keeps = jnp.where(lane == h, keep, keeps)
    keep_ref[...] = keeps


def update(state_ref, key_ref, correct_ref, keep_ref, after_ref, next_ref, token_ref, made_ref, sems):
    del after_ref
    copies = []
    for b in range(OWN):
        for h in range(HEADS_DEV):
            at = h * HEAD_DIM
            key_column = jnp.broadcast_to(key_ref[b : b + 1, at : at + HEAD_DIM], (128, 128)).T
            made_ref[b, h] = (
                keep_ref[b : b + 1, h : h + 1] * state_ref[b, h]
                + key_column * correct_ref[b : b + 1, at : at + HEAD_DIM]
            )
        copies.append(pltpu.make_async_copy(made_ref.at[b], next_ref.at[b], sems.at[b]))
        copies[-1].start()
    token_ref[...] = jnp.zeros(token_ref.shape, f32)
    for copy in copies:
        copy.wait()


def updated(*operands):
    return pl.pallas_call(
        update,
        out_shape=[shape(operands[0].shape, f32), shape((8, 128), f32)],
        in_specs=[in_vmem()] * 4 + [anywhere()],
        out_specs=[pl.BlockSpec(memory_space=pltpu.HBM), in_vmem()],
        scratch_shapes=[
            pltpu.VMEM((OWN, HEADS_DEV, HEAD_DIM, HEAD_DIM), f32),
            pltpu.SemaphoreType.DMA((OWN,)),
        ],
        name="update",
        compiler_params=pltpu.CompilerParams(vmem_limit_bytes=12 * 1024 * 1024),
    )(*operands)


def preload(*refs):
    count = (len(refs) - 1) // 2
    sems = refs[-1]
    copies = [
        pltpu.make_async_copy(refs[i], refs[count + i], sems.at[i]) for i in range(count)
    ]
    for copy in copies:
        copy.start()
    for copy in copies:
        copy.wait()


def preloaded(*arrays):
    return pl.pallas_call(
        preload,
        out_shape=[shape(x.shape, x.dtype) for x in arrays],
        in_specs=[pl.BlockSpec(memory_space=pltpu.HBM)] * len(arrays),
        out_specs=[in_vmem() for _ in arrays],
        scratch_shapes=[pltpu.SemaphoreType.DMA((len(arrays),))],
        name="preload",
        compiler_params=pltpu.CompilerParams(vmem_limit_bytes=4 * 1024 * 1024),
    )(*(pltpu.with_memory_space_constraint(x, pltpu.HBM) for x in arrays))


def note(after_ref, out_ref):
    del after_ref
    out_ref[...] = jnp.zeros(out_ref.shape, f32)


def join(held_ref, near_ref, rows_ref, after_ref, out_ref):
    del after_ref
    on_first = lax.axis_index("tp") == 0
    place = lax.axis_index("kv_1")
    out_ref[:WIDTH_DEV] = held_ref[:WIDTH_DEV]
    out_ref[WIDTH_DEV : 2 * WIDTH_DEV] = near_ref[:WIDTH_DEV]
    first = ring_tokens(rows_ref, jnp.bitwise_xor(place, 1), on_first, True)
    second = near_ref[WIDTH_DEV:].astype(f32)
    out_ref[2 * WIDTH_DEV :] = jnp.where(low_lanes(first), first, second).astype(bf16)


def ring_parts(received_ref, joined_ref):
    mixed = received_ref[...]
    parts = []
    for at in (0, WIDTH_DEV):
        both = dot(mixed, joined_ref[at : at + WIDTH_DEV])
        parts.append(both[:SEQ_RING] + half_turn(both[SEQ_RING:]))
    return parts


def mix(received_ref, joined_ref, near_ref, far_ref, rows_ref, after_ref, sent_ref):
    del after_ref
    on_first = lax.axis_index("tp") == 0
    place = lax.axis_index("kv_1")
    held, third = ring_parts(received_ref, joined_ref)
    first, second = ring_parts(received_ref, far_ref)
    far_tokens = far_ref[2 * WIDTH_DEV :].astype(f32)
    parts = [
        held + ring_tokens(rows_ref, place, on_first, True),
        first + far_tokens,
        second + half_turn(far_tokens),
        third + near_ref[WIDTH_DEV:].astype(f32),
    ]

    def part(column):
        which = jnp.bitwise_xor(place, column)
        value = parts[0]
        for m in range(1, RING):
            value = jnp.where(which == m, parts[m], value)
        return value

    low = low_lanes(parts[0])
    middle = jnp.concatenate(
        [jnp.where(low, part(c), half_turn(part(c + 1))) for c in range(0, RING, 2)], axis=1
    ).astype(bf16)
    for s in range(GROUP):
        sent_ref[SEQ_RING * s : SEQ_RING * (s + 1)] = middle


def gate_up(received_ref, gain_ref, wg_ref, wu_ref, own_ref, sent_ref, middle_ref, rows_ref):
    for s in range(GROUP):
        ring, place = s // RING, s % RING
        for r in range(RING):
            rows_ref[
                SEQ_RING * r + OWN * place : SEQ_RING * r + OWN * (place + 1),
                FEAT_RING * ring : FEAT_RING * (ring + 1),
            ] = received_ref[SEQ_RING * s + OWN * r : SEQ_RING * s + OWN * (r + 1)]
    middle = rows_ref[...].astype(f32)
    normed = (middle * gain_ref[0:1]).astype(bf16)
    for at, ref in ((0, wg_ref), (HIDDEN, wu_ref)):
        value = dot(ref[...], normed, NT)
        own_ref[at : at + HIDDEN] = value
        sent_ref[at : at + HIDDEN] = value.astype(bf16)
    squares = jnp.sum(middle * middle, axis=1, keepdims=True)
    total = jnp.broadcast_to(squares, (ROWS, 128)).T[0:1]
    high, low = high_low(total)
    own_ref[BOTH:] = jnp.broadcast_to(total, (8, ROWS))
    sent_ref[BOTH:] = jnp.concatenate([high, low, jnp.zeros((6, ROWS), f32)], axis=0).astype(bf16)
    place = lax.axis_index("kv_1")
    pair = lax.axis_index("kv_0") * 2 + jnp.right_shift(place, 1)
    block = rows_ref[:, pl.ds(pl.multiple_of(pair * 128, 128), 128)].astype(f32).T
    even = jnp.bitwise_and(place, 1) == 0
    middle_ref[...] = jnp.where(even, block[:FEAT], block[FEAT:]).astype(bf16)


def down(own_ref, other_ref, w_ref, after_ref, out_ref):
    del after_ref
    squares = other_ref[BOTH:].astype(f32)
    total = own_ref[BOTH : BOTH + 1] + squares[0:1] + squares[1:2]
    scale = lax.rsqrt(total / D + norm_epsilon)
    gate = (own_ref[:HIDDEN] + other_ref[:HIDDEN].astype(f32)) * scale
    up = (own_ref[HIDDEN:BOTH] + other_ref[HIDDEN:BOTH].astype(f32)) * scale
    active = (silu(gate) * up).astype(bf16)
    out_ref[...] = dot(w_ref[...], active, TN).astype(bf16)


def finish(received_ref, middle_ref, out_ref):
    parts = [received_ref[FEAT * s : FEAT * (s + 1)].astype(f32) for s in range(GROUP)]
    while len(parts) > 1:
        parts = [a + b for a, b in zip(parts[::2], parts[1::2])]
    out_ref[...] = (middle_ref[...].astype(f32) + parts[0]).astype(bf16)


def from_other_core(array):
    return lax.ppermute(array, "tp", [(0, 1), (1, 0)])


def over(array, axes, members):
    tiles = array.reshape(members, array.shape[0] // members, array.shape[1])
    return lax.all_to_all(tiles, axes, 0, 0, tiled=True).reshape(array.shape)


def from_ring(array, flip):
    return lax.ppermute(array, "kv_1", [(i, i ^ flip) for i in range(RING)])


def layer(
    tokens,
    delta_state,
    gain_in,
    w_query,
    w_key,
    w_value,
    w_out_gate,
    w_beta,
    w_decay,
    decay_rate,
    head_gain,
    w_mix,
    gain_mid,
    w_gate,
    w_up,
    w_down,
):
    v, a = in_vmem(), anywhere()
    own_tokens = tokens.T
    other_tokens = from_other_core(own_tokens)
    other_mix = from_other_core(w_mix)
    loaded = preloaded(
        own_tokens,
        gain_in.reshape(1, 128),
        gain_mid.reshape(1, 128),
        w_query,
        w_key,
        w_value,
        w_out_gate,
        w_beta.T,
        w_decay.T,
        w_mix,
    )
    summand, rows, held = kernel(
        project,
        [shape((ROWS, PIECE), bf16), shape((ROWS, 128), bf16), shape((PACKED, 128), bf16)],
        [v] * 12,
    )(*loaded, other_tokens, other_mix)
    near = from_ring(held, 3)
    pieces = over(summand, KV, GROUP)
    mark = kernel(note, shape((8, 128), f32), [a])(pieces)
    joined = kernel(join, shape((JOINED, 128), bf16), [v] * 3 + [a])(
        held, near, rows, mark
    )
    far = from_ring(joined, 1)
    mixed, key, correction, keep, gains = kernel(
        mixer,
        [
            shape((2 * RING * OWN, WIDTH_DEV), bf16),
            shape((OWN, WIDTH_DEV), f32),
            shape((OWN, WIDTH_DEV), f32),
            shape((OWN, HEAD_DIM), f32),
            shape((OWN, GROUP * FEAT), f32),
        ],
        [v] * 4,
    )(pieces, delta_state, decay_rate.reshape(1, HEADS_DEV), head_gain.reshape(1, HEAD_DIM))
    mixed_rows = over(mixed, ("tp", "kv_0"), 2 * RING)
    arrived = kernel(note, shape((8, 128), f32), [a])(mixed_rows)
    sent = kernel(mix, shape((GROUP * SEQ_RING, FEAT_RING), bf16), [v] * 5 + [a])(
        mixed_rows, joined, near, far, rows, arrived
    )
    received = over(sent, KV, GROUP)
    own_sum, sent_sum, middle = pl.pallas_call(
        gate_up,
        out_shape=[
            shape((BOTH + 8, ROWS), f32),
            shape((BOTH + 8, ROWS), bf16),
            shape((FEAT, ROWS), bf16),
        ],
        in_specs=[v] * 4,
        out_specs=[v] * 3,
        scratch_shapes=[pltpu.VMEM((ROWS, GROUP * FEAT), bf16)],
        name="gate_up",
        compiler_params=pltpu.CompilerParams(vmem_limit_bytes=12 * 1024 * 1024),
    )(received, gains, w_gate.T, w_up.T)
    next_state, token = updated(delta_state, key, correction, keep, received)
    down_local = kernel(down, shape((GROUP * FEAT, ROWS), bf16), [v, v, v, a])(
        own_sum, from_other_core(sent_sum), w_down, token
    )
    layer_out = kernel(finish, shape((FEAT, ROWS), bf16), [v] * 2)(
        over(down_local, KV, GROUP), middle
    )
    return (layer_out.T, next_state)


def solution(mesh):
    split = Mesh(
        mesh.devices.reshape(mesh.shape["dp"], 4, 4, mesh.shape["tp"]), ("dp", "kv_0", "kv_1", "tp")
    )
    in_specs = (
        P("dp", KV_TP),
        P(DP_KV, "tp", None, None),
        P(KV),
        P(KV, "tp"),
        P(KV, "tp"),
        P(KV, "tp"),
        P(KV, "tp"),
        P(KV, None),
        P(KV, None),
        P("tp"),
        P(),
        P("tp", KV),
        P(KV),
        P("tp", KV),
        P("tp", KV),
        P(KV, "tp"),
    )
    out_specs = (P("dp", KV_TP), P(DP_KV, "tp", None, None))
    return jax.shard_map(layer, mesh=split, in_specs=in_specs, out_specs=out_specs, check_vma=False)
```

```python
import jax
import jax.numpy as jnp
from jax import lax
from jax.experimental import pallas as pl
from jax.experimental.pallas import tpu as pltpu
from jax.sharding import Mesh
from jax.sharding import PartitionSpec as P


D = 2048
HEAD_DIM = 128
KV = ("kv_0", "kv_1")
KV_TP = ("kv_0", "kv_1", "tp")
DP_KV = ("dp", "kv_0", "kv_1")

norm_epsilon = 1e-06
bf16 = jnp.bfloat16
f32 = jnp.float32

GROUP = 16
ROWS = 128
OWN = ROWS // GROUP
FEAT = 64
HEADS_DEV = 4
WIDTH_DEV = HEADS_DEV * HEAD_DIM
SMALL_AT = 4 * WIDTH_DEV
PIECE = SMALL_AT + 128
RING = 4
FEAT_RING = RING * FEAT
SEQ_RING = RING * OWN
PACKED = WIDTH_DEV + SEQ_RING
JOINED = 2 * WIDTH_DEV + SEQ_RING
HIDDEN = 352
BOTH = 2 * HIDDEN

TN = (((0,), (0,)), ((), ()))
NT = (((1,), (1,)), ((), ()))


def in_vmem():
    return pl.BlockSpec(memory_space=pltpu.VMEM)


def anywhere():
    return pl.BlockSpec(memory_space=pl.ANY)


def shape(lengths, dtype):
    return jax.ShapeDtypeStruct(lengths, dtype)


def kernel(body, outs, in_specs, limit=12):
    single = not isinstance(outs, (list, tuple))
    return pl.pallas_call(
        body,
        out_shape=outs,
        in_specs=in_specs,
        out_specs=in_vmem() if single else [in_vmem() for _ in outs],
        compiler_params=pltpu.CompilerParams(vmem_limit_bytes=limit * 1024 * 1024),
    )


def silu(value):
    return value / (1.0 + jnp.exp(-value))


def high_low(value):
    high = value.astype(bf16).astype(f32)
    return high, value - high


def dot(left, right, dims=(((1,), (0,)), ((), ()))):
    return lax.dot_general(left, right, dims, preferred_element_type=f32)


def half_turn(value):
    return pltpu.roll(value, 64, 1)


def project(
    own_ref, gain_ref, gain_mid_ref, wq_ref, wk_ref, wv_ref, wg_ref, wb_ref, wd_ref, own_mix_ref, other_ref, other_mix_ref, out_ref, rows_ref, held_ref, joined_ref
):
    on_first = lax.axis_index("tp") == 0
    own = own_ref[...].astype(f32)
    other = other_ref[...].astype(f32)
    rows = jnp.concatenate(
        [jnp.where(on_first, own, other), jnp.where(on_first, other, own)], axis=0
    ).T
    rows_ref[...] = rows.astype(bf16)
    high, low = high_low(jnp.sum(rows * rows, axis=1, keepdims=True))
    normed = (rows * gain_ref[...].astype(f32)).astype(bf16)
    for at, ref in enumerate((wq_ref, wk_ref, wv_ref, wg_ref)):
        out_ref[:, at * WIDTH_DEV : (at + 1) * WIDTH_DEV] = dot(normed, ref[...]).astype(bf16)
    beta = wb_ref[...].astype(f32)
    decay = wd_ref[...].astype(f32)
    small = jnp.concatenate(
        [
            jnp.where(on_first, beta[:HEADS_DEV], beta[HEADS_DEV:]),
            jnp.where(on_first, decay[:HEADS_DEV], decay[HEADS_DEV:]),
            jnp.zeros((128 - 2 * HEADS_DEV, 128), f32),
        ],
        axis=0,
    ).astype(bf16)
    extra = dot(normed, small, NT)
    lane = lax.broadcasted_iota(jnp.int32, extra.shape, 1)
    gain_mid = jnp.broadcast_to(gain_mid_ref[...].astype(f32), extra.shape)
    gain_mid = jnp.where(on_first, half_turn(gain_mid), gain_mid)
    extra = jnp.where(lane == 2 * HEADS_DEV, high, extra)
    extra = jnp.where(lane == 2 * HEADS_DEV + 1, low, extra)
    out_ref[:, SMALL_AT:] = jnp.where(lane >= 64, gain_mid, extra).astype(bf16)
    pack(own_mix_ref, other_mix_ref, rows_ref, held_ref)
    joined_ref[:WIDTH_DEV] = held_ref[:WIDTH_DEV]
    near_place = jnp.bitwise_xor(lax.axis_index("kv_1"), 1)
    joined_ref[2 * WIDTH_DEV :] = ring_tokens(rows_ref, near_place, on_first, True).astype(bf16)


def low_lanes(value):
    return lax.broadcasted_iota(jnp.int32, value.shape, 1) < 64


def ring_tokens(rows_ref, place, on_first, low):
    parts = [
        rows_ref[pl.ds(pl.multiple_of(SEQ_RING * r + OWN * place, OWN), OWN)].astype(f32)
        for r in range(RING)
    ]
    value = jnp.concatenate(parts, axis=0)
    turned = half_turn(value)
    return jnp.where(on_first, value, turned) if low else jnp.where(on_first, turned, value)


def pack(own_ref, other_ref, rows_ref, out_ref):
    on_first = lax.axis_index("tp") == 0
    place = lax.axis_index("kv_1")
    own = own_ref[...].astype(f32)
    other = other_ref[...].astype(f32)
    top = jnp.where(on_first, own, half_turn(other))
    bottom = jnp.where(on_first, half_turn(other), own)
    out_ref[:WIDTH_DEV] = jnp.where(low_lanes(own), top, bottom).astype(bf16)
    first = ring_tokens(rows_ref, jnp.bitwise_xor(place, 3), on_first, True)
    second = ring_tokens(rows_ref, jnp.bitwise_xor(place, 2), on_first, False)
    out_ref[WIDTH_DEV:] = jnp.where(low_lanes(first), first, second).astype(bf16)


def mixer(
    pieces_ref,
    state_ref,
    rate_ref,
    head_gain_ref,
    mixed_ref,
    key_ref,
    correct_ref,
    keep_ref,
    gain_ref,
):
    def total(first, last):
        parts = [pieces_ref[OWN * s : OWN * (s + 1), first:last].astype(f32) for s in range(GROUP)]
        while len(parts) > 1:
            parts = [a + b for a, b in zip(parts[::2], parts[1::2])]
        return parts[0]

    def block(s, at):
        return pieces_ref[OWN * s : OWN * (s + 1), at : at + 128].astype(f32)

    small = total(SMALL_AT, PIECE)
    lane = lax.broadcasted_iota(jnp.int32, (OWN, HEAD_DIM), 1)
    squares = jnp.where((lane == 2 * HEADS_DEV) | (lane == 2 * HEADS_DEV + 1), small, 0.0)
    row_scale = lax.rsqrt(jnp.sum(squares, axis=1, keepdims=True) / D + norm_epsilon)
    small = small * row_scale
    own = jnp.bitwise_and(lax.broadcasted_iota(jnp.int32, (2 * OWN, HEAD_DIM), 0), OWN - 1)
    keeps = jnp.zeros((OWN, HEAD_DIM), f32)
    low = lane < 64
    for s in range(0, GROUP, 2):
        gain_ref[:, FEAT * s : FEAT * (s + 2)] = jnp.where(
            low, half_turn(block(s, SMALL_AT)), block(s + 1, SMALL_AT)
        )

    def unit(vector):
        return vector * lax.rsqrt(jnp.sum(vector * vector, axis=1, keepdims=True) + norm_epsilon)

    for h in range(HEADS_DEV):
        at = h * HEAD_DIM
        query_lin, key_lin, value_lin, gate_lin = (
            total(part * WIDTH_DEV + at, part * WIDTH_DEV + at + HEAD_DIM) * row_scale
            for part in range(4)
        )
        query = unit(silu(query_lin)) * HEAD_DIM ** (-0.5)
        key = unit(silu(key_lin))
        write_rate = 1.0 / (1.0 + jnp.exp(-small[:, h : h + 1]))
        decay = small[:, HEADS_DEV + h : HEADS_DEV + h + 1]
        softplus = jnp.maximum(decay, 0.0) + jnp.log1p(jnp.exp(-jnp.abs(decay)))
        keep = jnp.exp(-rate_ref[:, h : h + 1] * softplus)
        pair = jnp.concatenate([key, query], axis=0)
        spread = jnp.concatenate([jnp.where(own == b, pair, 0.0) for b in range(OWN)], axis=1)
        states = state_ref[:, h].reshape(OWN * HEAD_DIM, HEAD_DIM)
        both = dot(spread.astype(bf16), states.astype(bf16))
        recalled, asked = both[:OWN], both[OWN:]
        correction = write_rate * (silu(value_lin) - keep * recalled)
        readout = keep * asked + jnp.sum(key * query, axis=1, keepdims=True) * correction
        readout = readout * lax.rsqrt(
            jnp.mean(readout * readout, axis=1, keepdims=True) + norm_epsilon
        )
        mixed = (readout * head_gain_ref[...] * silu(gate_lin)).astype(bf16)
        for e in range(2 * RING):
            mixed_ref[OWN * e : OWN * (e + 1), at : at + HEAD_DIM] = mixed
        key_ref[:, at : at + HEAD_DIM] = key
        correct_ref[:, at : at + HEAD_DIM] = correction
        keeps = jnp.where(lane == h, keep, keeps)
    keep_ref[...] = keeps


def update(state_ref, key_ref, correct_ref, keep_ref, after_ref, next_ref, token_ref, made_ref, sems):
    del after_ref
    copies = []
    for b in range(OWN):
        for h in range(HEADS_DEV):
            at = h * HEAD_DIM
            key_column = jnp.broadcast_to(key_ref[b : b + 1, at : at + HEAD_DIM], (128, 128)).T
            made_ref[b, h] = (
                keep_ref[b : b + 1, h : h + 1] * state_ref[b, h]
                + key_column * correct_ref[b : b + 1, at : at + HEAD_DIM]
            )
        copies.append(pltpu.make_async_copy(made_ref.at[b], next_ref.at[b], sems.at[b]))
        copies[-1].start()
    token_ref[...] = jnp.zeros(token_ref.shape, f32)
    for copy in copies:
        copy.wait()


def updated(*operands):
    return pl.pallas_call(
        update,
        out_shape=[shape(operands[0].shape, f32), shape((8, 128), f32)],
        in_specs=[in_vmem()] * 4 + [anywhere()],
        out_specs=[pl.BlockSpec(memory_space=pltpu.HBM), in_vmem()],
        scratch_shapes=[
            pltpu.VMEM((OWN, HEADS_DEV, HEAD_DIM, HEAD_DIM), f32),
            pltpu.SemaphoreType.DMA((OWN,)),
        ],
        name="update",
        compiler_params=pltpu.CompilerParams(vmem_limit_bytes=12 * 1024 * 1024),
    )(*operands)


def preload(*refs):
    count = (len(refs) - 1) // 2
    sems = refs[-1]
    copies = [
        pltpu.make_async_copy(refs[i], refs[count + i], sems.at[i]) for i in range(count)
    ]
    for copy in copies:
        copy.start()
    for copy in copies:
        copy.wait()


def preloaded(*arrays):
    return pl.pallas_call(
        preload,
        out_shape=[shape(x.shape, x.dtype) for x in arrays],
        in_specs=[pl.BlockSpec(memory_space=pltpu.HBM)] * len(arrays),
        out_specs=[in_vmem() for _ in arrays],
        scratch_shapes=[pltpu.SemaphoreType.DMA((len(arrays),))],
        name="preload",
        compiler_params=pltpu.CompilerParams(vmem_limit_bytes=4 * 1024 * 1024),
    )(*(pltpu.with_memory_space_constraint(x, pltpu.HBM) for x in arrays))


def note(after_ref, out_ref):
    del after_ref
    out_ref[...] = jnp.zeros(out_ref.shape, f32)


def join(base_ref, near_ref, after_ref, out_ref):
    del after_ref
    first = base_ref[2 * WIDTH_DEV :].astype(f32)
    second = near_ref[WIDTH_DEV:].astype(f32)
    out_ref[WIDTH_DEV : 2 * WIDTH_DEV] = near_ref[:WIDTH_DEV]
    out_ref[2 * WIDTH_DEV :] = jnp.where(low_lanes(first), first, second).astype(bf16)


def ring_parts(received_ref, joined_ref):
    mixed = received_ref[...]
    parts = []
    for at in (0, WIDTH_DEV):
        both = dot(mixed, joined_ref[at : at + WIDTH_DEV])
        parts.append(both[:SEQ_RING] + half_turn(both[SEQ_RING:]))
    return parts


def mix(received_ref, joined_ref, near_ref, far_ref, rows_ref, after_ref, sent_ref):
    del after_ref
    on_first = lax.axis_index("tp") == 0
    place = lax.axis_index("kv_1")
    held, third = ring_parts(received_ref, joined_ref)
    first, second = ring_parts(received_ref, far_ref)
    far_tokens = far_ref[2 * WIDTH_DEV :].astype(f32)
    parts = [
        held + ring_tokens(rows_ref, place, on_first, True),
        first + far_tokens,
        second + half_turn(far_tokens),
        third + near_ref[WIDTH_DEV:].astype(f32),
    ]

    def part(column):
        which = jnp.bitwise_xor(place, column)
        value = parts[0]
        for m in range(1, RING):
            value = jnp.where(which == m, parts[m], value)
        return value

    low = low_lanes(parts[0])
    middle = jnp.concatenate(
        [jnp.where(low, part(c), half_turn(part(c + 1))) for c in range(0, RING, 2)], axis=1
    ).astype(bf16)
    for s in range(GROUP):
        sent_ref[SEQ_RING * s : SEQ_RING * (s + 1)] = middle


def gate_up(received_ref, gain_ref, wg_ref, wu_ref, own_ref, sent_ref, middle_ref, rows_ref):
    for s in range(GROUP):
        ring, place = s // RING, s % RING
        for r in range(RING):
            rows_ref[
                SEQ_RING * r + OWN * place : SEQ_RING * r + OWN * (place + 1),
                FEAT_RING * ring : FEAT_RING * (ring + 1),
            ] = received_ref[SEQ_RING * s + OWN * r : SEQ_RING * s + OWN * (r + 1)]
    middle = rows_ref[...].astype(f32)
    normed = (middle * gain_ref[0:1]).astype(bf16)
    for at, ref in ((0, wg_ref), (HIDDEN, wu_ref)):
        value = dot(ref[...], normed, NT)
        own_ref[at : at + HIDDEN] = value
        sent_ref[at : at + HIDDEN] = value.astype(bf16)
    squares = jnp.sum(middle * middle, axis=1, keepdims=True)
    total = jnp.broadcast_to(squares, (ROWS, 128)).T[0:1]
    high, low = high_low(total)
    own_ref[BOTH:] = jnp.broadcast_to(total, (8, ROWS))
    sent_ref[BOTH:] = jnp.concatenate([high, low, jnp.zeros((6, ROWS), f32)], axis=0).astype(bf16)
    place = lax.axis_index("kv_1")
    pair = lax.axis_index("kv_0") * 2 + jnp.right_shift(place, 1)
    block = rows_ref[:, pl.ds(pl.multiple_of(pair * 128, 128), 128)].astype(f32).T
    even = jnp.bitwise_and(place, 1) == 0
    middle_ref[...] = jnp.where(even, block[:FEAT], block[FEAT:]).astype(bf16)


def down(own_ref, other_ref, w_ref, after_ref, out_ref):
    del after_ref
    squares = other_ref[BOTH:].astype(f32)
    total = own_ref[BOTH : BOTH + 1] + squares[0:1] + squares[1:2]
    scale = lax.rsqrt(total / D + norm_epsilon)
    gate = (own_ref[:HIDDEN] + other_ref[:HIDDEN].astype(f32)) * scale
    up = (own_ref[HIDDEN:BOTH] + other_ref[HIDDEN:BOTH].astype(f32)) * scale
    active = (silu(gate) * up).astype(bf16)
    out_ref[...] = dot(w_ref[...], active, TN).astype(bf16)


def finish(received_ref, middle_ref, out_ref):
    parts = [received_ref[FEAT * s : FEAT * (s + 1)].astype(f32) for s in range(GROUP)]
    while len(parts) > 1:
        parts = [a + b for a, b in zip(parts[::2], parts[1::2])]
    out_ref[...] = (middle_ref[...].astype(f32) + parts[0]).astype(bf16)


def from_other_core(array):
    return lax.ppermute(array, "tp", [(0, 1), (1, 0)])


def over(array, axes, members):
    tiles = array.reshape(members, array.shape[0] // members, array.shape[1])
    return lax.all_to_all(tiles, axes, 0, 0, tiled=True).reshape(array.shape)


def from_ring(array, flip):
    return lax.ppermute(array, "kv_1", [(i, i ^ flip) for i in range(RING)])


def layer(
    tokens,
    delta_state,
    gain_in,
    w_query,
    w_key,
    w_value,
    w_out_gate,
    w_beta,
    w_decay,
    decay_rate,
    head_gain,
    w_mix,
    gain_mid,
    w_gate,
    w_up,
    w_down,
):
    v, a = in_vmem(), anywhere()
    own_tokens = tokens.T
    other_tokens = from_other_core(own_tokens)
    other_mix = from_other_core(w_mix)
    loaded = preloaded(
        own_tokens,
        gain_in.reshape(1, 128),
        gain_mid.reshape(1, 128),
        w_query,
        w_key,
        w_value,
        w_out_gate,
        w_beta.T,
        w_decay.T,
        w_mix,
    )
    summand, rows, held, base = kernel(
        project,
        [
            shape((ROWS, PIECE), bf16),
            shape((ROWS, 128), bf16),
            shape((PACKED, 128), bf16),
            shape((JOINED, 128), bf16),
        ],
        [v] * 12,
    )(*loaded, other_tokens, other_mix)
    near = from_ring(held, 3)
    pieces = over(summand, KV, GROUP)
    mark = kernel(note, shape((8, 128), f32), [a])(pieces)
    joined = pl.pallas_call(
        join,
        out_shape=shape((JOINED, 128), bf16),
        in_specs=[v, v, anywhere()],
        out_specs=v,
        input_output_aliases={0: 0},
        name="join",
        compiler_params=pltpu.CompilerParams(vmem_limit_bytes=12 * 1024 * 1024),
    )(base, near, mark)
    far = from_ring(joined, 1)
    mixed, key, correction, keep, gains = kernel(
        mixer,
        [
            shape((2 * RING * OWN, WIDTH_DEV), bf16),
            shape((OWN, WIDTH_DEV), f32),
            shape((OWN, WIDTH_DEV), f32),
            shape((OWN, HEAD_DIM), f32),
            shape((OWN, GROUP * FEAT), f32),
        ],
        [v] * 4,
    )(pieces, delta_state, decay_rate.reshape(1, HEADS_DEV), head_gain.reshape(1, HEAD_DIM))
    mixed_rows = over(mixed, ("tp", "kv_0"), 2 * RING)
    arrived = kernel(note, shape((8, 128), f32), [a])(mixed_rows)
    sent = kernel(mix, shape((GROUP * SEQ_RING, FEAT_RING), bf16), [v] * 5 + [a])(
        mixed_rows, joined, near, far, rows, arrived
    )
    received = over(sent, KV, GROUP)
    own_sum, sent_sum, middle = pl.pallas_call(
        gate_up,
        out_shape=[
            shape((BOTH + 8, ROWS), f32),
            shape((BOTH + 8, ROWS), bf16),
            shape((FEAT, ROWS), bf16),
        ],
        in_specs=[v] * 4,
        out_specs=[v] * 3,
        scratch_shapes=[pltpu.VMEM((ROWS, GROUP * FEAT), bf16)],
        name="gate_up",
        compiler_params=pltpu.CompilerParams(vmem_limit_bytes=12 * 1024 * 1024),
    )(received, gains, w_gate.T, w_up.T)
    next_state, token = updated(delta_state, key, correction, keep, received)
    down_local = kernel(down, shape((GROUP * FEAT, ROWS), bf16), [v, v, v, a])(
        own_sum, from_other_core(sent_sum), w_down, token
    )
    layer_out = kernel(finish, shape((FEAT, ROWS), bf16), [v] * 2)(
        over(down_local, KV, GROUP), middle
    )
    return (layer_out.T, next_state)


def solution(mesh):
    split = Mesh(
        mesh.devices.reshape(mesh.shape["dp"], 4, 4, mesh.shape["tp"]), ("dp", "kv_0", "kv_1", "tp")
    )
    in_specs = (
        P("dp", KV_TP),
        P(DP_KV, "tp", None, None),
        P(KV),
        P(KV, "tp"),
        P(KV, "tp"),
        P(KV, "tp"),
        P(KV, "tp"),
        P(KV, None),
        P(KV, None),
        P("tp"),
        P(),
        P("tp", KV),
        P(KV),
        P("tp", KV),
        P("tp", KV),
        P(KV, "tp"),
    )
    out_specs = (P("dp", KV_TP), P(DP_KV, "tp", None, None))
    return jax.shard_map(layer, mesh=split, in_specs=in_specs, out_specs=out_specs, check_vma=False)
```
